256 devices in a mesh: sp: 64 (over z, x, core), tp: 4 (over y).
Axes of the slice: x: 4, y: 4, z: 8, core: 2. Of those that a mesh axis runs over, the one named last changes fastest.
Arguments:
- q_first: bfloat16 [12288, 512], P('sp', 'tp'), may hold values from -6 to 6
- k_first: bfloat16 [12288, 512], P('sp', 'tp'), may hold values from -6 to 6
- q_second: bfloat16 [12288, 512], P('sp', 'tp'), may hold values from -6 to 6
- k_second: bfloat16 [12288, 512], P('sp', 'tp'), may hold values from -6 to 6
- values: bfloat16 [12288, 1024], P('sp', 'tp'), may hold values from -6 to 6
- lambdas: float32 [8], P('tp'), may hold values from 0.3 to 0.8
- head_gain: float32 [128], replicated, may hold values from 0.1 to 1.9
- out_weight: bfloat16 [1024, 2048], P('tp'), may hold values from -0.1875 to 0.1875
- residual_in: bfloat16 [12288, 2048], P('sp'), may hold values from -6 to 6
- mix_gain: float32 [2048], replicated, may hold values from 0.1 to 1.9
- gate_weight: bfloat16 [2048, 5632], P('sp', 'tp'), may hold values from -0.125 to 0.125
- up_weight: bfloat16 [2048, 5632], P('sp', 'tp'), may hold values from -0.125 to 0.125
- gate_taps: float32 [3, 5632], P(None, 'tp'), may hold values from -3.5 to 3.5
- up_taps: float32 [3, 5632], P(None, 'tp'), may hold values from -3.5 to 3.5
- down_weight: bfloat16 [5632, 2048], P('tp'), may hold values from -0.078125 to 0.078125
Outputs:
- mixed: bfloat16 [12288, 2048], P(('sp', 'tp'))
The draws below stay inside these ranges and needn't reach their ends.
All inputs are finite; a program needn't handle non-finite values.
Results may differ from the reference program's by a relative error of at most 0.017.
Values may be sent and summed in bfloat16 or wider, within the bound.
A program may use at most 128 MiB of HBM per device.

```python
import math
import jax
import jax.numpy as jnp
from jax import lax

D = 2048
HEADS = 8
HEAD_DIM = 64
VALUE_DIM = 128
FF = 5632
KERNEL = 3
TOKENS = 12288


def aligned_pair(key):
    shape = (TOKENS, HEADS * HEAD_DIM)
    query_key = jax.random.fold_in(key, 71)
    other_key = jax.random.fold_in(key, 72)
    queries = jnp.clip(1.35 * jax.random.normal(query_key, shape, jnp.float32), -6.0, 6.0)
    keys = jnp.clip(1.35 * jax.random.normal(other_key, shape, jnp.float32), -6.0, 6.0)
    return (queries.astype(jnp.bfloat16), keys.astype(jnp.bfloat16))


def draw_q_first(key, part):
    return aligned_pair(key)[0]


def draw_k_first(key, part):
    return aligned_pair(key)[1]


def shard_levels(own_key, extent, pieces, low, top_value):
    loudness = 1.0
    for position, shards_of in pieces:
        heights = jax.random.uniform(jax.random.fold_in(jax.random.fold_in(own_key, 6), position), (shards_of,), jnp.float32, low / len(pieces), top_value / len(pieces))
        loudness = loudness * jnp.repeat(jnp.exp(heights), extent[position] // shards_of).reshape((-1,) + (1,) * (len(extent) - 1 - position))
    return loudness


def normal_values(key, dims, spread, limit, split=(), kind=jnp.bfloat16):
    entries = spread * jax.random.normal(key, dims, jnp.float32)
    if split:
        entries = entries * shard_levels(key, dims, split, -0.22, 0.18)
    return jnp.clip(entries, -limit, limit).astype(kind)


def setup_inputs(seed: int = 0) -> dict:
    arg_keys = jax.random.split(jax.random.key(seed), 16)
    return {
        "q_first": draw_q_first(jax.random.fold_in(arg_keys[15], 71), 0),
        "k_first": draw_k_first(jax.random.fold_in(arg_keys[15], 71), 0),
        "q_second": normal_values(arg_keys[2], (TOKENS, HEADS * HEAD_DIM), 1.35, 6.0, ((0, 64), (1, 4))),
        "k_second": normal_values(arg_keys[3], (TOKENS, HEADS * HEAD_DIM), 1.35, 6.0, ((0, 64), (1, 4))),
        "values": normal_values(arg_keys[4], (TOKENS, HEADS * VALUE_DIM), 1.0, 6.0, ((0, 64), (1, 4))),
        "lambdas": jnp.clip(0.3 + 0.5 * jax.random.uniform(arg_keys[5], (HEADS,), jnp.float32) ** shard_levels(arg_keys[5], (HEADS,), ((0, 4),), -0.2, 0.2), 0.3, 0.8),
        "head_gain": jnp.clip(1.0 + 0.18 * jax.random.normal(arg_keys[6], (VALUE_DIM,), jnp.float32), 0.1, 1.9),
        "out_weight": normal_values(arg_keys[7], (HEADS * VALUE_DIM, D), (HEADS * VALUE_DIM) ** -0.5, 0.1875, ((0, 4),)),
        "residual_in": normal_values(arg_keys[8], (TOKENS, D), 1.0, 6.0, ((0, 64),)),
        "mix_gain": jnp.clip(1.0 + 0.18 * jax.random.normal(arg_keys[9], (D,), jnp.float32), 0.1, 1.9),
        "gate_weight": normal_values(arg_keys[10], (D, FF), D ** -0.5, 0.125, ((0, 64), (1, 4))),
        "up_weight": normal_values(arg_keys[11], (D, FF), D ** -0.5, 0.125, ((0, 64), (1, 4))),
        "gate_taps": normal_values(arg_keys[12], (KERNEL, FF), KERNEL ** -0.5, 3.5, ((1, 4),), jnp.float32),
        "up_taps": normal_values(arg_keys[13], (KERNEL, FF), KERNEL ** -0.5, 3.5, ((1, 4),), jnp.float32),
        "down_weight": normal_values(arg_keys[14], (FF, D), FF ** -0.5, 0.078125, ((0, 4),)),
    }


norm_eps = 1e-06
far_below = -1e+30

def reference(q_first, k_first, q_second, k_second, values, lambdas, head_gain, out_weight, residual_in, mix_gain, gate_weight, up_weight, gate_taps, up_taps, down_weight):
    total = q_first.shape[0]
    scale = HEAD_DIM ** (-0.5)
    query_a = q_first.astype(jnp.float32).reshape(total, HEADS, HEAD_DIM)
    query_b = q_second.astype(jnp.float32).reshape(total, HEADS, HEAD_DIM)
    keys_a = k_first.astype(jnp.float32).reshape(total, HEADS, HEAD_DIM)
    keys_b = k_second.astype(jnp.float32).reshape(total, HEADS, HEAD_DIM)
    vals = values.astype(jnp.float32).reshape(total, HEADS, VALUE_DIM)
    block_rows = math.gcd(total, 512)
    key_pos = jnp.arange(total, dtype=jnp.int32)

    def weigh(queries, keys, visible):
        scores = jnp.einsum('qhd,khd->hqk', queries, keys, precision=lax.Precision.HIGHEST) * scale
        masked = jnp.where(visible, scores, far_below)
        peak = lax.optimization_barrier(jnp.max(masked, axis=-1, keepdims=True))
        expo = jnp.where(visible, jnp.exp(masked - peak), 0.0)
        totals = lax.optimization_barrier(jnp.sum(expo, axis=-1))
        rounded = expo.astype(jnp.bfloat16).astype(jnp.float32)
        accum = jnp.einsum('hqk,khv->qhv', rounded, vals, precision=lax.Precision.HIGHEST)
        return accum / totals.T[..., None]

    def attend(block_index):
        row_start = (block_index * block_rows).astype(jnp.int32)
        query_pos = row_start + jnp.arange(block_rows, dtype=jnp.int32)
        visible = (key_pos[None, :] <= query_pos[:, None])[None]
        first = weigh(lax.dynamic_slice_in_dim(query_a, row_start, block_rows, 0), keys_a, visible)
        second = weigh(lax.dynamic_slice_in_dim(query_b, row_start, block_rows, 0), keys_b, visible)
        diff_heads = first - lambdas[None, :, None] * second
        normed = diff_heads * lax.rsqrt(lax.optimization_barrier(jnp.mean(diff_heads * diff_heads, axis=-1, keepdims=True)) + norm_eps) * head_gain
        return normed.astype(jnp.bfloat16).reshape(block_rows, HEADS * VALUE_DIM)
    head_out = lax.map(attend, jnp.arange(total // block_rows, dtype=jnp.int32)).reshape(total, HEADS * VALUE_DIM)
    attended = jnp.dot(head_out, out_weight, preferred_element_type=jnp.float32)
    stream = residual_in.astype(jnp.float32) + attended
    ffn_in = (stream * lax.rsqrt(lax.optimization_barrier(jnp.mean(stream * stream, axis=-1, keepdims=True)) + norm_eps) * mix_gain).astype(jnp.bfloat16)
    gate_pre = jnp.dot(ffn_in, gate_weight, preferred_element_type=jnp.float32).astype(jnp.bfloat16)
    up_pre = jnp.dot(ffn_in, up_weight, preferred_element_type=jnp.float32).astype(jnp.bfloat16)

    def convolve(projected, taps):
        padded = jnp.pad(projected.astype(jnp.float32), ((KERNEL - 1, 0), (0, 0)))
        result = taps[0][None, :] * padded[0:total]
        for offset in range(1, KERNEL):
            result = result + taps[offset][None, :] * padded[offset:offset + total]
        return result
    gate_conv = convolve(gate_pre, gate_taps)
    up_conv = convolve(up_pre, up_taps)
    hidden = (jax.nn.silu(gate_conv) * up_conv).astype(jnp.bfloat16)
    return (stream + jnp.dot(hidden, down_weight, preferred_element_type=jnp.float32)).astype(jnp.bfloat16)
```

```python
import functools

import jax
import jax.numpy as jnp
from jax import lax
from jax.experimental import pallas as pl
from jax.experimental.pallas import tpu as pltpu
from jax.sharding import PartitionSpec as P

MESH = pl.DeviceIdType.MESH
norm_eps = 1e-06
ROWS = 192
NX, NZ, NY = 4, 8, 4
DX = (2, 1, 3)
HIDE = -2e30
FLOOR = -1e30
f32, bf16 = jnp.float32, jnp.bfloat16


def rms_scale(field, gain):
    return field * lax.rsqrt(jnp.mean(field * field, axis=-1, keepdims=True) + norm_eps) * gain


def attention_kernel(
    qa, qb, ka, kb, va, gw, uw, lam, gain,
    head_out, wg_out, wu_out,
    q, kv, wg, wu, qz, m, l, acc, psend, precv, ssend, srecv,
    loc, bar_q, kvs, kvr, kds, kdr, wus, wur, wxs, wxr, wds, wdr, gxs, gxr, gzs, gzr, gds, gdr, pts, ptr, sts, str_,
):
    r = lax.axis_index("sp")
    y = lax.axis_index("tp")
    z, x, c = r // 8, (r // 2) % 4, r % 2

    def at(zz, xx, cc):
        return (lax.rem(zz + NZ, NZ) * 8 + lax.rem(xx + NX, NX) * 2 + cc, y)

    mate = (r + 1 - 2 * c, y)
    up_dev, down_dev = at(z + 1, x, c), at(z - 1, x, c)

    def rcopy(src, dst, ss, rs, dev):
        return pltpu.make_async_remote_copy(
            src_ref=src, dst_ref=dst, send_sem=ss, recv_sem=rs, device_id=dev, device_id_type=MESH
        )

    loads = [
        (qa, q.at[x, :, 0:128]),
        (qb, q.at[x, :, 128:256]),
        (ka, kv.at[z, c, :, 0:128]),
        (kb, kv.at[z, c, :, 128:256]),
        (va, kv.at[z, c, :, 256:512]),
        (gw, wg.at[z, x, c]),
        (uw, wu.at[z, x, c]),
    ]
    loads = [pltpu.make_async_copy(s, d, loc.at[i]) for i, (s, d) in enumerate(loads)]
    for d in loads:
        d.start()
    barrier = pltpu.get_barrier_semaphore()
    for dev in [up_dev, down_dev, mate] + [at(z, x + d, c) for d in DX]:
        pl.semaphore_signal(barrier, inc=1, device_id=dev, device_id_type=MESH)
    pl.semaphore_wait(barrier, 6)
    for d in loads:
        d.wait()

    def q_copy(i, slot):
        return rcopy(q.at[slot], q.at[slot], bar_q.at[0, i], bar_q.at[1, i], at(z, x + DX[i], c))

    plus_n, minus_n = 4 - c, 3 + c

    def z_ring(ref_at, sends, recvs):
        def plus(s):
            blk = lax.rem(z - s + 1 + NZ, NZ)
            return rcopy(ref_at(blk), ref_at(blk), sends.at[0, s - 1], recvs.at[0, s - 1], up_dev)

        def minus(s):
            blk = lax.rem(z + s - 1, NZ)
            return rcopy(ref_at(blk), ref_at(blk), sends.at[1, s - 1], recvs.at[1, s - 1], down_dev)

        def plus_in(s):
            blk = lax.rem(z - s + NZ, NZ)
            return rcopy(ref_at(blk), ref_at(blk), sends.at[0, s - 1], recvs.at[0, s - 1], up_dev)

        def minus_in(s):
            blk = lax.rem(z + s, NZ)
            return rcopy(ref_at(blk), ref_at(blk), sends.at[1, s - 1], recvs.at[1, s - 1], down_dev)

        return plus, minus, plus_in, minus_in

    def only(n, s, fn):
        if s <= 3:
            fn()
        elif s == 4:
            pl.when(n == 4)(fn)

    kv_ring = z_ring(lambda b: kv.at[b, c], kvs, kvr)
    wu_ring = z_ring(lambda b: wu.at[b, x, c], wus, wur)
    wg_ring = z_ring(lambda b: wg.at[b, :, c], gzs, gzr)

    def hand_blk(k):
        off = (0, -1, -2, -3, 1, 2, 3, 4)[k]
        return lax.rem(z + off + NZ, NZ)

    def kv_hand(k, lane):
        b = hand_blk(k)
        return rcopy(kv.at[b, lane], kv.at[b, lane], kds.at[k], kdr.at[k], mate)

    def wg_hand(k, lane):
        b = hand_blk(k)
        return rcopy(wg.at[b, :, lane], wg.at[b, :, lane], gds.at[k], gdr.at[k], mate)

    def wu_hand(k, lane):
        b = hand_blk(k)
        return rcopy(wu.at[b, :, lane], wu.at[b, :, lane], wds.at[k], wdr.at[k], mate)

    def wu_x(k, i, xx):
        b = hand_blk(k)
        return rcopy(wu.at[b, xx, c], wu.at[b, xx, c], wxs.at[k, i], wxr.at[k, i], at(z, x + DX[i], c))

    def wg_x(i, xx):
        return rcopy(wg.at[z, xx, c], wg.at[z, xx, c], gxs.at[i], gxr.at[i], at(z, x + DX[i], c))

    def from_x(i):
        return lax.rem(x - DX[i] + NX, NX)

    def ring_start(ring):
        ring[0](1).start()
        ring[1](1).start()

    def ring_step(ring, s, hand):
        def p():
            ring[2](s).wait_recv()
            only(plus_n, s + 1, lambda: ring[0](s + 1).start())
            if s < 4:
                hand(s)
            else:
                hand(7)

        def n():
            ring[3](s).wait_recv()
            only(minus_n, s + 1, lambda: ring[1](s + 1).start())
            if s < 4:
                hand(3 + s)
            else:
                hand(7)

        only(plus_n, s, p)
        only(minus_n, s, n)

    def ks(s):
        return (s, 3 + s) if s < 4 else (7,)

    for i in range(3):
        q_copy(i, x).start()
    ring_start(kv_ring)
    kv_hand(0, c).start()
    for i in range(3):
        wg_x(i, x).start()
    ring_start(wu_ring)
    for i in range(3):
        wu_x(0, i, x).start()

    m[...] = jnp.full_like(m, FLOOR)
    l[...] = jnp.zeros_like(l)
    acc[...] = jnp.zeros_like(acc)

    lane = lax.broadcasted_iota(jnp.int32, (ROWS, 128), 1)

    def prepare(slot):
        for half in range(2):
            block = q[slot, :, half * 128 : (half + 1) * 128] * bf16(0.125)
            zero = jnp.zeros_like(block)
            qz[half, slot, 0:ROWS] = jnp.where(lane < 64, block, zero)
            qz[half, slot, ROWS : 2 * ROWS] = jnp.where(lane < 64, zero, block)

    prepare(x)
    for i in range(3):
        q_copy(i, from_x(i)).wait_recv()
        prepare(from_x(i))

    def piece(pair, slot, masked):
        if masked:
            j = lax.broadcasted_iota(jnp.int32, (1, 768), 1)
            second = (j >= 384).astype(jnp.int32)
            core = ((j - 384 * second) >= 192).astype(jnp.int32)
            off = j - 384 * second - 192 * core
            key_pos = ((2 * pair + second) * 8 + x * 2 + core) * ROWS + off
            i = lax.broadcasted_iota(jnp.int32, (2 * ROWS, 1), 0)
            i = i - ROWS * (i >= ROWS).astype(jnp.int32)
            query_pos = (z * 8 + slot * 2 + c) * ROWS + i
            visible = key_pos <= query_pos
        for half in range(2):
            keys = kv[pl.ds(2 * pair, 2), :, :, half * 128 : (half + 1) * 128].reshape(768, 128)
            s = lax.dot_general(
                qz[half, slot], keys, (((1,), (1,)), ((), ())), preferred_element_type=f32
            )
            if masked:
                s = jnp.where(visible, s, HIDE)
            old = m[half, slot]
            new = jnp.maximum(old, jnp.max(s, axis=1, keepdims=True))
            fade = jnp.exp(old - new)
            m[half, slot] = new
            e = jnp.exp(s - new[:, 0:1])
            part = e[:, 0:128]
            for t in range(1, 6):
                part = part + e[:, t * 128 : (t + 1) * 128]
            l[half, slot] = l[half, slot] * fade + part
            eb = e.astype(bf16)
            for h in range(2):
                rows = slice(h * ROWS, (h + 1) * ROWS)
                vals = kv[pl.ds(2 * pair, 2), :, :, 256 + h * 128 : 384 + h * 128].reshape(768, 128)
                acc[half, slot, rows] = acc[half, slot, rows] * fade[rows] + jnp.dot(
                    eb[rows], vals, preferred_element_type=f32
                )

    own = z // 2
    odd = z % 2
    pairs = (
        own,
        lax.rem(own + jnp.where(odd == 1, 1, 3), 4),
        lax.rem(own + jnp.where(odd == 1, 3, 1), 4),
        lax.rem(own + 2, 4),
    )

    def sum_stats(slot):
        st = jnp.zeros((ROWS, 128), f32)
        for half in range(2):
            for h in range(2):
                rows = slice(h * ROWS, (h + 1) * ROWS)
                k = half * 2 + h
                st = jnp.where(lane == k, m[half, slot, rows], st)
                tot = jnp.sum(l[half, slot, rows], axis=1, keepdims=True)
                st = jnp.where(lane == 4 + k, tot, st)
        return st

    def p_copy(i):
        return rcopy(psend.at[i], precv.at[i], pts.at[i], ptr.at[i], (at(z, x + i_dx(i), c)))

    def s_copy(i):
        return rcopy(ssend.at[i], srecv.at[i], sts.at[i], str_.at[i], (at(z, x + i_dx(i), c)))

    def i_dx(i):
        return jnp.where(i == 0, 2, jnp.where(i == 1, 1, 3))

    wu_hand_waits = []
    for ci in range(4):
        s = ci + 1
        ring_step(kv_ring, s, lambda k: kv_hand(k, c).start())
        if ci == 0:
            kv_hand(0, 1 - c).wait_recv()
        for k in ks(s):
            kv_hand(k, 1 - c).wait_recv()
        pair = pairs[ci]
        if ci == 0:
            def body0(slot, carry):
                piece(pair, slot, True)
                return carry
            lax.fori_loop(0, 4, body0, 0)
        elif ci < 3:
            @pl.when(pair < own)
            def _():
                def body1(slot, carry):
                    piece(pair, slot, False)
                    return carry
                lax.fori_loop(0, 4, body1, 0)
        else:
            def body3(i, carry):
                slot = lax.rem(x + jnp.where(i == 3, 0, i_dx(i)), NX)

                @pl.when(pair < own)
                def _():
                    piece(pair, slot, False)

                @pl.when(i < 3)
                def _():
                    for half in range(2):
                        for h in range(2):
                            col = (half * 2 + h) * 128
                            psend[i, :, col : col + 128] = acc[
                                half, slot, h * ROWS : (h + 1) * ROWS
                            ].astype(bf16)
                    st = jnp.concatenate((sum_stats(slot), jnp.zeros((64, 128), f32)), axis=0)
                    ssend[i] = st.T[0:8]
                    p_copy(i).start()
                    s_copy(i).start()
                return carry
            lax.fori_loop(0, 4, body3, 0)

        ring_step(
            wu_ring, s,
            (lambda k: [wu_x(k, i, x).start() for i in range(3)]),
        )
        if ci == 0:
            for i in range(3):
                wg_x(i, from_x(i)).wait_recv()
            wg_hand(0, c).start()
        if ci == 1:
            for i in range(3):
                wu_x(0, i, from_x(i)).wait_recv()
            wu_hand(0, c).start()
            for k in ks(1):
                for i in range(3):
                    wu_x(k, i, from_x(i)).wait_recv()
                wu_hand(k, c).start()
        if ci == 2:
            ring_start(wg_ring)

    ring_step(wg_ring, 1, lambda k: wg_hand(k, c).start())

    def take(i):
        p_copy(i).wait_recv()
        s_copy(i).wait_recv()
        st = jnp.concatenate((srecv[i], jnp.zeros((120, 256), f32)), axis=0).T[0:ROWS]
        return st

    stats = [sum_stats(x)] + [take(i) for i in range(3)]
    for h in range(2):
        parts = []
        for half in range(2):
            k = half * 2 + h
            col = k * 128
            ms = [st[:, k : k + 1] for st in stats]
            ls = [st[:, 4 + k : 5 + k] for st in stats]
            top = functools.reduce(jnp.maximum, ms)
            ws = [jnp.exp(a - top) for a in ms]
            tot = sum(w * t for w, t in zip(ws, ls))
            out = acc[half, x, h * ROWS : (h + 1) * ROWS] * ws[0]
            for i in range(3):
                out = out + precv[i, :, col : col + 128].astype(f32) * ws[i + 1]
            parts.append(out / tot)
        diff = parts[0] - lam[h : h + 1, :] * parts[1]
        head_out[:, h * 128 : (h + 1) * 128] = rms_scale(diff, gain[...]).astype(bf16)

    def wu_finish(k):
        for i in range(3):
            wu_x(k, i, from_x(i)).wait_recv()
        wu_hand(k, c).start()

    for k in ks(2):
        wu_finish(k)
    ring_step(wg_ring, 2, lambda k: wg_hand(k, c).start())
    for k in ks(3):
        wu_finish(k)
    ring_step(wg_ring, 3, lambda k: wg_hand(k, c).start())
    wu_finish(7)
    ring_step(wg_ring, 4, lambda k: wg_hand(k, c).start())
    for k in range(8):
        wg_hand(k, 1 - c).wait_recv()
        wu_hand(k, 1 - c).wait_recv()

    a = pltpu.make_async_copy(wg, wg_out, loc.at[0])
    b = pltpu.make_async_copy(wu, wu_out, loc.at[1])
    a.start()
    b.start()

    for i in range(3):
        q_copy(i, x).wait_send()
        wg_x(i, x).wait_send()
        p_copy(i).wait_send()
        s_copy(i).wait_send()
    for ring in (kv_ring, wu_ring, wg_ring):
        for s in range(1, 5):
            only(plus_n, s, lambda: ring[0](s).wait_send())
            only(minus_n, s, lambda: ring[1](s).wait_send())
    for k in range(8):
        kv_hand(k, c).wait_send()
        wg_hand(k, c).wait_send()
        wu_hand(k, c).wait_send()
        for i in range(3):
            wu_x(k, i, x).wait_send()
    a.wait()
    b.wait()


def attention(qa, qb, ka, kb, va, gw, uw, lam, gain):
    ANY = pl.BlockSpec(memory_space=pl.ANY)
    VM = pl.BlockSpec(memory_space=pltpu.VMEM)
    ff = gw.shape[1]
    dma = pltpu.SemaphoreType.DMA
    return pl.pallas_call(
        attention_kernel,
        out_shape=(
            jax.ShapeDtypeStruct((ROWS, 256), bf16),
            jax.ShapeDtypeStruct((8, 4, 2, 32, ff), bf16),
            jax.ShapeDtypeStruct((8, 4, 2, 32, ff), bf16),
        ),
        in_specs=[ANY] * 7 + [VM, VM],
        out_specs=(VM, ANY, ANY),
        scratch_shapes=[
            pltpu.VMEM((4, ROWS, 256), bf16),
            pltpu.VMEM((8, 2, ROWS, 512), bf16),
            pltpu.VMEM((8, 4, 2, 32, ff), bf16),
            pltpu.VMEM((8, 4, 2, 32, ff), bf16),
            pltpu.VMEM((2, 4, 2 * ROWS, 128), bf16),
            pltpu.VMEM((2, 4, 2 * ROWS, 128), f32),
            pltpu.VMEM((2, 4, 2 * ROWS, 128), f32),
            pltpu.VMEM((2, 4, 2 * ROWS, 128), f32),
            pltpu.VMEM((3, ROWS, 512), bf16),
            pltpu.VMEM((3, ROWS, 512), bf16),
            pltpu.VMEM((3, 8, 256), f32),
            pltpu.VMEM((3, 8, 256), f32),
            dma((7,)),
            dma((2, 3)),
            dma((2, 4)),
            dma((2, 4)),
            dma((8,)),
            dma((8,)),
            dma((2, 4)),
            dma((2, 4)),
            dma((8, 3)),
            dma((8, 3)),
            dma((8,)),
            dma((8,)),
            dma((3,)),
            dma((3,)),
            dma((2, 4)),
            dma((2, 4)),
            dma((8,)),
            dma((8,)),
            dma((3,)),
            dma((3,)),
            dma((3,)),
            dma((3,)),
        ],
        compiler_params=pltpu.CompilerParams(
            collective_id=0, has_side_effects=True, vmem_limit_bytes=60 * 1024 * 1024
        ),
        name="attend",
    )(qa, qb, ka, kb, va, gw, uw, lam, gain)


def split_up(array, dim, devices):
    dims = array.shape
    blocks = array.reshape(*dims[:dim], devices, dims[dim] // devices, *dims[dim + 1 :])
    return jnp.moveaxis(blocks, dim, 0)


def sent_and_summed(array, axis, dim):
    blocks = split_up(array, dim, lax.axis_size(axis))
    arrived = lax.all_to_all(blocks, axis, split_axis=0, concat_axis=0, tiled=True)
    return arrived.astype(jnp.float32).sum(axis=0)


def passed_along(value, axis, steps):
    count = lax.axis_size(axis)
    initial, last = (max(0, -steps), min(count, count - steps))
    return lax.ppermute(value, axis, [(source, source + steps) for source in range(initial, last)])


def shards(
    q_first, k_first, q_second, k_second, values, lambdas, head_gain, out_weight, residual_in,
    mix_gain, gate_weight, up_weight, gate_taps, up_taps, down_weight,
):
    tok_rows = q_first.shape[0]
    part_rows = tok_rows // lax.axis_size("tp")
    tp_rank = lax.axis_index("tp")
    lam = jnp.broadcast_to(lambdas[:, None], (2, 128))
    head_out, gate_full, up_full = attention(
        q_first, q_second, k_first, k_second, values, gate_weight, up_weight, lam, head_gain[None]
    )
    gate_full = gate_full.reshape(2048, -1)
    up_full = up_full.reshape(2048, -1)
    attended = sent_and_summed(
        jnp.dot(head_out, out_weight, preferred_element_type=jnp.float32).astype(jnp.bfloat16),
        "tp",
        0,
    )
    own_rows = lax.dynamic_slice_in_dim(residual_in, tp_rank * part_rows, part_rows, 0)
    stream_rows = own_rows.astype(jnp.float32) + attended
    normed_part = rms_scale(stream_rows, mix_gain).astype(jnp.bfloat16)
    ffn_in = lax.all_gather(normed_part, "tp", axis=0, tiled=True)
    gate_pre = jnp.dot(ffn_in, gate_full, preferred_element_type=jnp.float32)
    up_pre = jnp.dot(ffn_in, up_full, preferred_element_type=jnp.float32)
    projected = jnp.stack((gate_pre.astype(jnp.bfloat16), up_pre.astype(jnp.bfloat16)))
    tap_count = gate_taps.shape[0]
    edge = passed_along(projected[:, tok_rows - (tap_count - 1) :], "sp", 1)
    padded = jnp.concatenate((edge, projected), axis=1).astype(jnp.float32)
    taps = jnp.stack((gate_taps, up_taps))
    convolved = taps[:, 0][:, None, :] * padded[:, 0:tok_rows]
    for offset in range(1, tap_count):
        convolved = convolved + taps[:, offset][:, None, :] * padded[:, offset : offset + tok_rows]
    hidden = (jax.nn.silu(convolved[0]) * convolved[1]).astype(jnp.bfloat16)
    down_rows = sent_and_summed(
        jnp.dot(hidden, down_weight, preferred_element_type=jnp.float32).astype(jnp.bfloat16),
        "tp",
        0,
    )
    return (stream_rows + down_rows).astype(jnp.bfloat16)


def solution(mesh):
    in_specs = (
        P("sp", "tp"), P("sp", "tp"), P("sp", "tp"), P("sp", "tp"), P("sp", "tp"),
        P("tp"), P(), P("tp", None), P("sp", None), P(),
        P("sp", "tp"), P("sp", "tp"), P(None, "tp"), P(None, "tp"), P("tp", None),
    )
    out_specs = P(("sp", "tp"), None)
    return jax.shard_map(shards, mesh=mesh, in_specs=in_specs, out_specs=out_specs, check_vma=False)
```

```python
import functools

import jax
import jax.numpy as jnp
from jax import lax
from jax.experimental import pallas as pl
from jax.experimental.pallas import tpu as pltpu
from jax.sharding import PartitionSpec as P

MESH = pl.DeviceIdType.MESH
norm_eps = 1e-06
ROWS = 192
NX, NZ, NY = 4, 8, 4
DX = (2, 1, 3)
HIDE = -2e30
FLOOR = -1e30
f32, bf16 = jnp.float32, jnp.bfloat16


def rms_scale(field, gain):
    return field * lax.rsqrt(jnp.mean(field * field, axis=-1, keepdims=True) + norm_eps) * gain


def layer_kernel(
    qa, qb, ka, kb, va, gw, uw, out_w, res_in, down_w, lam, gain, mix_gain, gate_taps, up_taps,
    out,
    q, kv, wg, wu, qz, m, l, acc, psend, precv, ssend, srecv,
    heads, ow, dw, res, stream, ffn, gate_pad, up_pad, hidden, edge_out, edge_in, part, drecv,
    loc, bar_q, kvs, kvr, kds, kdr, wus, wur, wxs, wxr, wds, wdr, gxs, gxr, gzs, gzr, gds, gdr, pts, ptr, sts, str_,
    hys, hyr, oys, oyr, ods, odr, es, er, dys, dyr,
):
    r = lax.axis_index("sp")
    y = lax.axis_index("tp")
    z, x, c = r // 8, (r // 2) % 4, r % 2

    def at(zz, xx, cc):
        return (lax.rem(zz + NZ, NZ) * 8 + lax.rem(xx + NX, NX) * 2 + cc, y)

    mate = (r + 1 - 2 * c, y)
    up_dev, down_dev = at(z + 1, x, c), at(z - 1, x, c)

    def rcopy(src, dst, ss, rs, dev):
        return pltpu.make_async_remote_copy(
            src_ref=src, dst_ref=dst, send_sem=ss, recv_sem=rs, device_id=dev, device_id_type=MESH
        )

    loads = [
        (qa, q.at[x, :, 0:128]),
        (qb, q.at[x, :, 128:256]),
        (ka, kv.at[z, c, :, 0:128]),
        (kb, kv.at[z, c, :, 128:256]),
        (va, kv.at[z, c, :, 256:512]),
        (gw, wg.at[z, x, c]),
        (uw, wu.at[z, x, c]),
        (out_w, ow.at[y]),
        (res_in, res),
        (down_w, dw),
    ]
    loads = [pltpu.make_async_copy(s, d, loc.at[i]) for i, (s, d) in enumerate(loads)]
    for d in loads:
        d.start()
    barrier = pltpu.get_barrier_semaphore()
    across = [(r, lax.rem(y + d, NY)) for d in DX]
    after, before = (lax.rem(r + 1, 64), y), (lax.rem(r + 63, 64), y)
    greeted = [up_dev, down_dev, mate, after, before] + [at(z, x + d, c) for d in DX] + across
    for dev in greeted:
        pl.semaphore_signal(barrier, inc=1, device_id=dev, device_id_type=MESH)
    pl.semaphore_wait(barrier, len(greeted))
    for d in loads[:5]:
        d.wait()

    def q_copy(i, slot):
        return rcopy(q.at[slot], q.at[slot], bar_q.at[0, i], bar_q.at[1, i], at(z, x + DX[i], c))

    plus_n, minus_n = 4 - c, 3 + c

    def z_ring(ref_at, sends, recvs):
        def plus(s):
            blk = lax.rem(z - s + 1 + NZ, NZ)
            return rcopy(ref_at(blk), ref_at(blk), sends.at[0, s - 1], recvs.at[0, s - 1], up_dev)

        def minus(s):
            blk = lax.rem(z + s - 1, NZ)
            return rcopy(ref_at(blk), ref_at(blk), sends.at[1, s - 1], recvs.at[1, s - 1], down_dev)

        def plus_in(s):
            blk = lax.rem(z - s + NZ, NZ)
            return rcopy(ref_at(blk), ref_at(blk), sends.at[0, s - 1], recvs.at[0, s - 1], up_dev)

        def minus_in(s):
            blk = lax.rem(z + s, NZ)
            return rcopy(ref_at(blk), ref_at(blk), sends.at[1, s - 1], recvs.at[1, s - 1], down_dev)

        return plus, minus, plus_in, minus_in

    def only(n, s, fn):
        if s <= 3:
            fn()
        elif s == 4:
            pl.when(n == 4)(fn)

    kv_ring = z_ring(lambda b: kv.at[b, c], kvs, kvr)
    wu_ring = z_ring(lambda b: wu.at[b, x, c], wus, wur)
    wg_ring = z_ring(lambda b: wg.at[b, :, c], gzs, gzr)

    def hand_blk(k):
        off = (0, -1, -2, -3, 1, 2, 3, 4)[k]
        return lax.rem(z + off + NZ, NZ)

    def kv_hand(k, lane):
        b = hand_blk(k)
        return rcopy(kv.at[b, lane], kv.at[b, lane], kds.at[k], kdr.at[k], mate)

    def wg_hand(k, lane):
        b = hand_blk(k)
        return rcopy(wg.at[b, :, lane], wg.at[b, :, lane], gds.at[k], gdr.at[k], mate)

    def wu_hand(k, lane):
        b = hand_blk(k)
        return rcopy(wu.at[b, :, lane], wu.at[b, :, lane], wds.at[k], wdr.at[k], mate)

    def wu_x(k, i, xx):
        b = hand_blk(k)
        return rcopy(wu.at[b, xx, c], wu.at[b, xx, c], wxs.at[k, i], wxr.at[k, i], at(z, x + DX[i], c))

    def wg_x(i, xx):
        return rcopy(wg.at[z, xx, c], wg.at[z, xx, c], gxs.at[i], gxr.at[i], at(z, x + DX[i], c))

    def from_x(i):
        return lax.rem(x - DX[i] + NX, NX)

    def ring_start(ring):
        ring[0](1).start()
        ring[1](1).start()

    def ring_step(ring, s, hand):
        def p():
            ring[2](s).wait_recv()
            only(plus_n, s + 1, lambda: ring[0](s + 1).start())
            if s < 4:
                hand(s)
            else:
                hand(7)

        def n():
            ring[3](s).wait_recv()
            only(minus_n, s + 1, lambda: ring[1](s + 1).start())
            if s < 4:
                hand(3 + s)
            else:
                hand(7)

        only(plus_n, s, p)
        only(minus_n, s, n)

    def ks(s):
        return (s, 3 + s) if s < 4 else (7,)

    def from_y(i):
        return lax.rem(y - DX[i] + NY, NY)

    half_cols = ow.shape[2] // 2

    def ow_y(i, yy):
        ref = ow.at[yy, :, pl.ds(pl.multiple_of(c * half_cols, 128), half_cols)]
        return rcopy(ref, ref, oys.at[i], oyr.at[i], across[i])

    def ow_hand(i, lane):
        ref = ow.at[from_y(i), :, pl.ds(pl.multiple_of(lane * half_cols, 128), half_cols)]
        return rcopy(ref, ref, ods.at[i], odr.at[i], mate)

    def heads_y(i, yy):
        return rcopy(heads.at[yy], heads.at[yy], hys.at[i], hyr.at[i], across[i])

    def edge_copy():
        return rcopy(edge_out, edge_in, es, er, after)

    def down_y(i, n):
        return rcopy(
            part.at[n, across[i][1]], drecv.at[i, n], dys.at[i, n], dyr.at[i, n], across[i]
        )

    for i in range(3):
        q_copy(i, x).start()
    ring_start(kv_ring)
    kv_hand(0, c).start()
    for d in loads[5:8]:
        d.wait()
    for i in range(3):
        ow_y(i, y).start()
    for i in range(3):
        wg_x(i, x).start()
    ring_start(wu_ring)
    for i in range(3):
        wu_x(0, i, x).start()

    lane = lax.broadcasted_iota(jnp.int32, (ROWS, 128), 1)

    def prepare(slot):
        for half in range(2):
            block = q[slot, :, half * 128 : (half + 1) * 128] * bf16(0.125)
            zero = jnp.zeros_like(block)
            qz[half, slot, 0:ROWS] = jnp.where(lane < 64, block, zero)
            qz[half, slot, ROWS : 2 * ROWS] = jnp.where(lane < 64, zero, block)

    prepare(x)
    for i in range(3):
        q_copy(i, from_x(i)).wait_recv()
        prepare(from_x(i))

    def piece(pair, slot, masked):
        if masked:
            j = lax.broadcasted_iota(jnp.int32, (1, 768), 1)
            second = (j >= 384).astype(jnp.int32)
            core = ((j - 384 * second) >= 192).astype(jnp.int32)
            off = j - 384 * second - 192 * core
            key_pos = ((2 * pair + second) * 8 + x * 2 + core) * ROWS + off
            i = lax.broadcasted_iota(jnp.int32, (2 * ROWS, 1), 0)
            i = i - ROWS * (i >= ROWS).astype(jnp.int32)
            query_pos = (z * 8 + slot * 2 + c) * ROWS + i
            visible = key_pos <= query_pos
        for half in range(2):
            keys = kv[pl.ds(2 * pair, 2), :, :, half * 128 : (half + 1) * 128].reshape(768, 128)
            s = lax.dot_general(
                qz[half, slot], keys, (((1,), (1,)), ((), ())), preferred_element_type=f32
            )
            if masked:
                s = jnp.where(visible, s, HIDE)
            if masked:
                new = jnp.broadcast_to(
                    jnp.maximum(jnp.max(s, axis=1, keepdims=True), FLOOR), (2 * ROWS, 128)
                )
            else:
                old = m[half, slot]
                new = jnp.maximum(old, jnp.max(s, axis=1, keepdims=True))
                fade = jnp.exp(old - new)
            m[half, slot] = new
            e = jnp.exp(s - new[:, 0:1])
            part_sum = e[:, 0:128]
            for t in range(1, 6):
                part_sum = part_sum + e[:, t * 128 : (t + 1) * 128]
            l[half, slot] = part_sum if masked else l[half, slot] * fade + part_sum
            eb = e.astype(bf16)
            for h in range(2):
                rows = slice(h * ROWS, (h + 1) * ROWS)
                vals = kv[pl.ds(2 * pair, 2), :, :, 256 + h * 128 : 384 + h * 128].reshape(768, 128)
                more = jnp.dot(eb[rows], vals, preferred_element_type=f32)
                if masked:
                    acc[half, slot, rows] = more
                else:
                    acc[half, slot, rows] = acc[half, slot, rows] * fade[rows] + more

    own = z // 2
    odd = z % 2
    pairs = (
        own,
        lax.rem(own + jnp.where(odd == 1, 1, 3), 4),
        lax.rem(own + jnp.where(odd == 1, 3, 1), 4),
        lax.rem(own + 2, 4),
    )

    def sum_stats(slot):
        st = jnp.zeros((ROWS, 128), f32)
        for half in range(2):
            for h in range(2):
                rows = slice(h * ROWS, (h + 1) * ROWS)
                k = half * 2 + h
                st = jnp.where(lane == k, m[half, slot, rows], st)
                tot = jnp.sum(l[half, slot, rows], axis=1, keepdims=True)
                st = jnp.where(lane == 4 + k, tot, st)
        return st

    def p_copy(i):
        return rcopy(psend.at[i], precv.at[i], pts.at[i], ptr.at[i], (at(z, x + i_dx(i), c)))

    def s_copy(i):
        return rcopy(ssend.at[i], srecv.at[i], sts.at[i], str_.at[i], (at(z, x + i_dx(i), c)))

    def i_dx(i):
        return jnp.where(i == 0, 2, jnp.where(i == 1, 1, 3))

    wu_hand_waits = []
    for ci in range(4):
        s = ci + 1
        ring_step(kv_ring, s, lambda k: kv_hand(k, c).start())
        if ci == 0:
            kv_hand(0, 1 - c).wait_recv()
        for k in ks(s):
            kv_hand(k, 1 - c).wait_recv()
        pair = pairs[ci]
        if ci == 0:
            def body0(slot, carry):
                piece(pair, slot, True)
                return carry
            lax.fori_loop(0, 4, body0, 0)
        elif ci < 3:
            @pl.when(pair < own)
            def _():
                def body1(slot, carry):
                    piece(pair, slot, False)
                    return carry
                lax.fori_loop(0, 4, body1, 0)
        else:
            def body3(i, carry):
                slot = lax.rem(x + jnp.where(i == 3, 0, i_dx(i)), NX)

                @pl.when(pair < own)
                def _():
                    piece(pair, slot, False)

                @pl.when(i < 3)
                def _():
                    for half in range(2):
                        for h in range(2):
                            col = (half * 2 + h) * 128
                            psend[i, :, col : col + 128] = acc[
                                half, slot, h * ROWS : (h + 1) * ROWS
                            ].astype(bf16)
                    st = jnp.concatenate((sum_stats(slot), jnp.zeros((64, 128), f32)), axis=0)
                    ssend[i] = st.T[0:8]
                    p_copy(i).start()
                    s_copy(i).start()
                return carry
            lax.fori_loop(0, 4, body3, 0)

        ring_step(
            wu_ring, s,
            (lambda k: [wu_x(k, i, x).start() for i in range(3)]),
        )
        if ci == 0:
            for i in range(3):
                wg_x(i, from_x(i)).wait_recv()
            wg_hand(0, c).start()
        if ci == 1:
            for i in range(3):
                wu_x(0, i, from_x(i)).wait_recv()
            wu_hand(0, c).start()
            for k in ks(1):
                for i in range(3):
                    wu_x(k, i, from_x(i)).wait_recv()
                wu_hand(k, c).start()
        if ci == 2:
            ring_start(wg_ring)
            for i in range(3):
                ow_y(i, from_y(i)).wait_recv()
                ow_hand(i, c).start()

    ring_step(wg_ring, 1, lambda k: wg_hand(k, c).start())

    def take(i):
        p_copy(i).wait_recv()
        s_copy(i).wait_recv()
        st = jnp.concatenate((srecv[i], jnp.zeros((120, 256), f32)), axis=0).T[0:ROWS]
        return st

    stats = [sum_stats(x)] + [take(i) for i in range(3)]
    for h in range(2):
        parts = []
        for half in range(2):
            k = half * 2 + h
            col = k * 128
            ms = [st[:, k : k + 1] for st in stats]
            ls = [st[:, 4 + k : 5 + k] for st in stats]
            top = functools.reduce(jnp.maximum, ms)
            ws = [jnp.exp(a - top) for a in ms]
            tot = sum(w * t for w, t in zip(ws, ls))
            joined = acc[half, x, h * ROWS : (h + 1) * ROWS] * ws[0]
            for i in range(3):
                joined = joined + precv[i, :, col : col + 128].astype(f32) * ws[i + 1]
            parts.append(joined / tot)
        diff = parts[0] - lam[h] * parts[1]
        heads[y, :, h * 128 : (h + 1) * 128] = rms_scale(diff, gain[...]).astype(bf16)

    for i in range(3):
        heads_y(i, y).start()

    def wu_finish(k):
        for i in range(3):
            wu_x(k, i, from_x(i)).wait_recv()
        wu_hand(k, c).start()

    for k in ks(2):
        wu_finish(k)
    ring_step(wg_ring, 2, lambda k: wg_hand(k, c).start())

    loads[8].wait()
    loads[9].wait()
    for i in range(3):
        ow_hand(i, 1 - c).wait_recv()
    for i in range(3):
        heads_y(i, from_y(i)).wait_recv()
    width = stream.shape[2]
    for n in range(0, width, 512):
        cols = slice(n, n + 512)
        total = res[:, cols].astype(f32)
        for yy in range(NY):
            total = total + jnp.dot(heads[yy], ow[yy, :, cols], preferred_element_type=f32)
        stream[:, :, cols] = total.reshape(NY, ROWS // NY, 512)
    rows = stream[...].reshape(ROWS, width)
    ffn[...] = rms_scale(rows, mix_gain[...]).astype(bf16)

    for k in ks(3):
        wu_finish(k)
    ring_step(wg_ring, 3, lambda k: wg_hand(k, c).start())
    wu_finish(7)
    ring_step(wg_ring, 4, lambda k: wg_hand(k, c).start())
    for k in range(8):
        wu_hand(k, 1 - c).wait_recv()
    ff = hidden.shape[1]
    for n in range(0, ff, 256):
        cols = slice(n, min(n + 256, ff))
        w = wu[:, :, :, :, cols].reshape(width, -1)
        pre = jnp.dot(ffn[...], w, preferred_element_type=f32).astype(bf16).astype(f32)
        up_pad[8 : 8 + ROWS, cols] = pre
    for k in range(8):
        wg_hand(k, 1 - c).wait_recv()
    for n in range(0, ff, 256):
        cols = slice(n, min(n + 256, ff))
        w = wg[:, :, :, :, cols].reshape(width, -1)
        pre = jnp.dot(ffn[...], w, preferred_element_type=f32).astype(bf16).astype(f32)
        gate_pad[8 : 8 + ROWS, cols] = pre
    edge_out[0] = gate_pad[6 + ROWS : 8 + ROWS, :]
    edge_out[1] = up_pad[6 + ROWS : 8 + ROWS, :]
    edge_copy().start()

    def mix(top, size):
        for n in range(0, ff, 128):
            cols = slice(n, n + 128)
            conv = []
            for pad, taps in ((gate_pad, gate_taps), (up_pad, up_taps)):
                v = taps[0:1, cols] * pad[6 + top : 6 + top + size, cols]
                v = v + taps[1:2, cols] * pad[7 + top : 7 + top + size, cols]
                v = v + taps[2:3, cols] * pad[8 + top : 8 + top + size, cols]
                conv.append(v)
            hidden[top : top + size, cols] = (jax.nn.silu(conv[0]) * conv[1]).astype(bf16)

    mix(16, ROWS - 16)
    edge_copy().wait_recv()
    gate_pad[6:8, :] = jnp.where(r == 0, 0.0, edge_in[0])
    up_pad[6:8, :] = jnp.where(r == 0, 0.0, edge_in[1])
    mix(0, 16)

    for n in range(NY):
        cols = slice(n * 512, (n + 1) * 512)
        down = jnp.dot(hidden[...], dw[:, cols], preferred_element_type=f32)
        part[n] = down.astype(bf16).reshape(NY, ROWS // NY, 512)
        for i in range(3):
            down_y(i, n).start()
    for n in range(NY):
        cols = slice(n * 512, (n + 1) * 512)
        total = stream[y, :, cols] + part[n, y].astype(f32)
        for i in range(3):
            down_y(i, n).wait_recv()
            total = total + drecv[i, n].astype(f32)
        out[:, cols] = total.astype(bf16)

    edge_copy().wait_send()
    for i in range(3):
        q_copy(i, x).wait_send()
        wg_x(i, x).wait_send()
        p_copy(i).wait_send()
        s_copy(i).wait_send()
        ow_y(i, y).wait_send()
        ow_hand(i, c).wait_send()
        heads_y(i, y).wait_send()
        for n in range(NY):
            down_y(i, n).wait_send()
    for ring in (kv_ring, wu_ring, wg_ring):
        for s in range(1, 5):
            only(plus_n, s, lambda: ring[0](s).wait_send())
            only(minus_n, s, lambda: ring[1](s).wait_send())
    for k in range(8):
        kv_hand(k, c).wait_send()
        wg_hand(k, c).wait_send()
        wu_hand(k, c).wait_send()
        for i in range(3):
            wu_x(k, i, x).wait_send()


def layer(*args):
    ANY = pl.BlockSpec(memory_space=pl.ANY)
    VM = pl.BlockSpec(memory_space=pltpu.VMEM)
    SM = pl.BlockSpec(memory_space=pltpu.SMEM)
    ff, width = args[5].shape[1], args[8].shape[1]
    dma = pltpu.SemaphoreType.DMA
    sems = [(10,), (2, 3), (2, 4), (2, 4), (8,), (8,), (2, 4), (2, 4), (8, 3), (8, 3), (8,), (8,)]
    sems += [(3,), (3,), (2, 4), (2, 4), (8,), (8,), (3,), (3,), (3,), (3,)]
    sems += [(3,), (3,), (3,), (3,), (3,), (3,), None, None, (3, 4), (3, 4)]
    return pl.pallas_call(
        layer_kernel,
        out_shape=jax.ShapeDtypeStruct((ROWS // NY, width), bf16),
        in_specs=[ANY] * 10 + [SM] + [VM] * 4,
        out_specs=VM,
        scratch_shapes=[
            pltpu.VMEM((4, ROWS, 256), bf16),
            pltpu.VMEM((8, 2, ROWS, 512), bf16),
            pltpu.VMEM((8, 4, 2, 32, ff), bf16),
            pltpu.VMEM((8, 4, 2, 32, ff), bf16),
            pltpu.VMEM((2, 4, 2 * ROWS, 128), bf16),
            pltpu.VMEM((2, 4, 2 * ROWS, 128), f32),
            pltpu.VMEM((2, 4, 2 * ROWS, 128), f32),
            pltpu.VMEM((2, 4, 2 * ROWS, 128), f32),
            pltpu.VMEM((3, ROWS, 512), bf16),
            pltpu.VMEM((3, ROWS, 512), bf16),
            pltpu.VMEM((3, 8, 256), f32),
            pltpu.VMEM((3, 8, 256), f32),
            pltpu.VMEM((NY, ROWS, 256), bf16),
            pltpu.VMEM((NY, 256, width), bf16),
            pltpu.VMEM((ff, width), bf16),
            pltpu.VMEM((ROWS, width), bf16),
            pltpu.VMEM((NY, ROWS // NY, width), f32),
            pltpu.VMEM((ROWS, width), bf16),
            pltpu.VMEM((8 + ROWS, ff), f32),
            pltpu.VMEM((8 + ROWS, ff), f32),
            pltpu.VMEM((ROWS, ff), bf16),
            pltpu.VMEM((2, 2, ff), f32),
            pltpu.VMEM((2, 2, ff), f32),
            pltpu.VMEM((NY, NY, ROWS // NY, 512), bf16),
            pltpu.VMEM((3, NY, ROWS // NY, 512), bf16),
        ] + [dma if s is None else dma(s) for s in sems],
        compiler_params=pltpu.CompilerParams(
            collective_id=0, has_side_effects=True, vmem_limit_bytes=63 * 1024 * 1024
        ),
        name="layer",
    )(*args)


def shards(
    q_first, k_first, q_second, k_second, values, lambdas, head_gain, out_weight, residual_in,
    mix_gain, gate_weight, up_weight, gate_taps, up_taps, down_weight,
):
    return layer(
        q_first, q_second, k_first, k_second, values, gate_weight, up_weight, out_weight,
        residual_in, down_weight, lambdas, head_gain[None], mix_gain[None], gate_taps, up_taps,
    )


def solution(mesh):
    in_specs = (
        P("sp", "tp"), P("sp", "tp"), P("sp", "tp"), P("sp", "tp"), P("sp", "tp"),
        P("tp"), P(), P("tp", None), P("sp", None), P(),
        P("sp", "tp"), P("sp", "tp"), P(None, "tp"), P(None, "tp"), P("tp", None),
    )
    out_specs = P(("sp", "tp"), None)
    return jax.shard_map(shards, mesh=mesh, in_specs=in_specs, out_specs=out_specs, check_vma=False)
```

```python
import functools

import jax
import jax.numpy as jnp
from jax import lax
from jax.experimental import pallas as pl
from jax.experimental.pallas import tpu as pltpu
from jax.sharding import PartitionSpec as P

MESH = pl.DeviceIdType.MESH
norm_eps = 1e-06
ROWS = 192
NX, NZ, NY = 4, 8, 4
DX = (2, 1, 3)
HIDE = -2e30
FLOOR = -1e30
f32, bf16 = jnp.float32, jnp.bfloat16


def rms_scale(field, gain):
    return field * lax.rsqrt(jnp.mean(field * field, axis=-1, keepdims=True) + norm_eps) * gain


def layer_kernel(
    qa, qb, ka, kb, va, gw, uw, out_w, res_in, down_w, lam, gain, mix_gain, gate_taps, up_taps,
    out,
    q, kv, wg, wu, qz, m, l, acc, psend, precv, ssend, srecv,
    heads, ow, dw, res, stream, ffn, gate_pad, up_pad, hidden, edge_out, edge_in, part, drecv,
    loc, bar_q, kvs, kvr, kds, kdr, wus, wur, wxs, wxr, wds, wdr, gxs, gxr, gzs, gzr, gds, gdr, pts, ptr, sts, str_,
    hys, hyr, oys, oyr, ods, odr, es, er, dys, dyr,
):
    r = lax.axis_index("sp")
    y = lax.axis_index("tp")
    z, x, c = r // 8, (r // 2) % 4, r % 2

    def at(zz, xx, cc):
        return (lax.rem(zz + NZ, NZ) * 8 + lax.rem(xx + NX, NX) * 2 + cc, y)

    mate = (r + 1 - 2 * c, y)
    up_dev, down_dev = at(z + 1, x, c), at(z - 1, x, c)

    def rcopy(src, dst, ss, rs, dev):
        return pltpu.make_async_remote_copy(
            src_ref=src, dst_ref=dst, send_sem=ss, recv_sem=rs, device_id=dev, device_id_type=MESH
        )

    loads = [
        (qa, q.at[x, :, 0:128]),
        (qb, q.at[x, :, 128:256]),
        (ka, kv.at[z, c, :, 0:128]),
        (kb, kv.at[z, c, :, 128:256]),
        (va, kv.at[z, c, :, 256:512]),
        (gw, wg.at[z, x, c]),
        (uw, wu.at[z, x, c]),
        (out_w, ow.at[y]),
        (res_in, res),
        (down_w, dw),
    ]
    loads = [pltpu.make_async_copy(s, d, loc.at[i]) for i, (s, d) in enumerate(loads)]
    for d in loads:
        d.start()
    barrier = pltpu.get_barrier_semaphore()
    across = [(r, lax.rem(y + d, NY)) for d in DX]
    after, before = (lax.rem(r + 1, 64), y), (lax.rem(r + 63, 64), y)
    greeted = [up_dev, down_dev, mate, after, before] + [at(z, x + d, c) for d in DX] + across
    for dev in greeted:
        pl.semaphore_signal(barrier, inc=1, device_id=dev, device_id_type=MESH)
    pl.semaphore_wait(barrier, len(greeted))
    for d in loads[:5]:
        d.wait()

    def q_copy(i, slot):
        return rcopy(q.at[slot], q.at[slot], bar_q.at[0, i], bar_q.at[1, i], at(z, x + DX[i], c))

    plus_n, minus_n = 4 - c, 3 + c

    def z_ring(ref_at, sends, recvs):
        def plus(s):
            blk = lax.rem(z - s + 1 + NZ, NZ)
            return rcopy(ref_at(blk), ref_at(blk), sends.at[0, s - 1], recvs.at[0, s - 1], up_dev)

        def minus(s):
            blk = lax.rem(z + s - 1, NZ)
            return rcopy(ref_at(blk), ref_at(blk), sends.at[1, s - 1], recvs.at[1, s - 1], down_dev)

        def plus_in(s):
            blk = lax.rem(z - s + NZ, NZ)
            return rcopy(ref_at(blk), ref_at(blk), sends.at[0, s - 1], recvs.at[0, s - 1], up_dev)

        def minus_in(s):
            blk = lax.rem(z + s, NZ)
            return rcopy(ref_at(blk), ref_at(blk), sends.at[1, s - 1], recvs.at[1, s - 1], down_dev)

        return plus, minus, plus_in, minus_in

    def only(n, s, fn):
        if s <= 3:
            fn()
        elif s == 4:
            pl.when(n == 4)(fn)

    kv_ring = z_ring(lambda b: kv.at[b, c], kvs, kvr)
    wu_ring = z_ring(lambda b: wu.at[b, x, c], wus, wur)
    wg_rings = [
        z_ring(lambda b, j=j: wg.at[b, lax.rem(x + j, NX), c], gzs.at[j], gzr.at[j])
        for j in range(NX)
    ]

    def wg_step(j, s):
        ring_step(wg_rings[j], s, lambda k: None)
        if j == NX - 1:
            for k in ks(s):
                wg_hand(k, c).start()


    def hand_blk(k):
        off = (0, -1, -2, -3, 1, 2, 3, 4)[k]
        return lax.rem(z + off + NZ, NZ)

    def kv_hand(k, lane):
        b = hand_blk(k)
        return rcopy(kv.at[b, lane], kv.at[b, lane], kds.at[k], kdr.at[k], mate)

    def wg_hand(k, lane):
        b = hand_blk(k)
        return rcopy(wg.at[b, :, lane], wg.at[b, :, lane], gds.at[k], gdr.at[k], mate)

    def wu_hand(k, lane):
        b = hand_blk(k)
        return rcopy(wu.at[b, :, lane], wu.at[b, :, lane], wds.at[k], wdr.at[k], mate)

    def wu_x(k, i, xx):
        b = hand_blk(k)
        return rcopy(wu.at[b, xx, c], wu.at[b, xx, c], wxs.at[k, i], wxr.at[k, i], at(z, x + DX[i], c))

    def wg_x(i, xx):
        return rcopy(wg.at[z, xx, c], wg.at[z, xx, c], gxs.at[i], gxr.at[i], at(z, x + DX[i], c))

    def from_x(i):
        return lax.rem(x - DX[i] + NX, NX)

    def ring_start(ring):
        ring[0](1).start()
        ring[1](1).start()

    def ring_step(ring, s, hand):
        def p():
            ring[2](s).wait_recv()
            only(plus_n, s + 1, lambda: ring[0](s + 1).start())
            if s < 4:
                hand(s)
            else:
                hand(7)

        def n():
            ring[3](s).wait_recv()
            only(minus_n, s + 1, lambda: ring[1](s + 1).start())
            if s < 4:
                hand(3 + s)
            else:
                hand(7)

        only(plus_n, s, p)
        only(minus_n, s, n)

    def ks(s):
        return (s, 3 + s) if s < 4 else (7,)

    def from_y(i):
        return lax.rem(y - DX[i] + NY, NY)

    half_cols = ow.shape[2] // 2

    def ow_y(i, yy):
        ref = ow.at[yy, :, pl.ds(pl.multiple_of(c * half_cols, 128), half_cols)]
        return rcopy(ref, ref, oys.at[i], oyr.at[i], across[i])

    def ow_hand(i, lane):
        ref = ow.at[from_y(i), :, pl.ds(pl.multiple_of(lane * half_cols, 128), half_cols)]
        return rcopy(ref, ref, ods.at[i], odr.at[i], mate)

    def heads_y(i, yy):
        return rcopy(heads.at[yy], heads.at[yy], hys.at[i], hyr.at[i], across[i])

    def edge_copy():
        return rcopy(edge_out, edge_in, es, er, after)

    def down_y(i, n):
        return rcopy(
            part.at[n, across[i][1]], drecv.at[i, n], dys.at[i, n], dyr.at[i, n], across[i]
        )

    for i in range(3):
        q_copy(i, x).start()
    ring_start(kv_ring)
    kv_hand(0, c).start()
    for d in loads[5:8]:
        d.wait()
    for i in range(3):
        ow_y(i, y).start()
    ring_start(wu_ring)

    lane = lax.broadcasted_iota(jnp.int32, (ROWS, 128), 1)

    def prepare(slot):
        for half in range(2):
            block = q[slot, :, half * 128 : (half + 1) * 128] * bf16(0.125)
            zero = jnp.zeros_like(block)
            qz[half, slot, 0:ROWS] = jnp.where(lane < 64, block, zero)
            qz[half, slot, ROWS : 2 * ROWS] = jnp.where(lane < 64, zero, block)

    prepare(x)
    for i in (1, 2, 0):
        q_copy(i, from_x(i)).wait_recv()
    for i in range(3):
        wg_x(i, x).start()
    for i in range(3):
        wu_x(0, i, x).start()
    for i in range(3):
        prepare(from_x(i))

    def piece(chunk, pair, slot, masked):
        if masked:
            j = lax.broadcasted_iota(jnp.int32, (1, 768), 1)
            second = (j >= 384).astype(jnp.int32)
            core = ((j - 384 * second) >= 192).astype(jnp.int32)
            off = j - 384 * second - 192 * core
            key_pos = ((2 * pair + second) * 8 + x * 2 + core) * ROWS + off
            i = lax.broadcasted_iota(jnp.int32, (2 * ROWS, 1), 0)
            i = i - ROWS * (i >= ROWS).astype(jnp.int32)
            query_pos = (z * 8 + slot * 2 + c) * ROWS + i
            visible = key_pos <= query_pos
        for half in range(2):
            keys = kv[pl.ds(2 * pair, 2), :, :, half * 128 : (half + 1) * 128].reshape(768, 128)
            s = lax.dot_general(
                qz[half, slot], keys, (((1,), (1,)), ((), ())), preferred_element_type=f32
            )
            if masked:
                s = jnp.where(visible, s, HIDE)
            new = jnp.broadcast_to(
                jnp.maximum(jnp.max(s, axis=1, keepdims=True), FLOOR), (2 * ROWS, 128)
            )
            m[chunk, half, slot] = new
            e = jnp.exp(s - new[:, 0:1])
            part_sum = e[:, 0:128]
            for t in range(1, 6):
                part_sum = part_sum + e[:, t * 128 : (t + 1) * 128]
            l[chunk, half, slot] = part_sum
            eb = e.astype(bf16)
            for h in range(2):
                rows = slice(h * ROWS, (h + 1) * ROWS)
                vals = kv[pl.ds(2 * pair, 2), :, :, 256 + h * 128 : 384 + h * 128].reshape(768, 128)
                acc[chunk, half, slot, rows] = jnp.dot(eb[rows], vals, preferred_element_type=f32)

    def unseen(chunk, slot):
        for half in range(2):
            m[chunk, half, slot] = jnp.full((2 * ROWS, 128), FLOOR, f32)
            l[chunk, half, slot] = jnp.zeros((2 * ROWS, 128), f32)
            acc[chunk, half, slot] = jnp.zeros((2 * ROWS, 128), f32)

    own = z // 2
    odd = z % 2
    pairs = (
        own,
        lax.rem(own + jnp.where(odd == 1, 1, 3), 4),
        lax.rem(own + jnp.where(odd == 1, 3, 1), 4),
        lax.rem(own + 2, 4),
    )

    def join(slot, take_values):
        st = jnp.zeros((ROWS, 128), f32)
        for half in range(2):
            for h in range(2):
                rows = slice(h * ROWS, (h + 1) * ROWS)
                k = half * 2 + h
                ms = [m[n, half, slot, rows] for n in range(4)]
                top = jnp.maximum(jnp.maximum(ms[0], ms[1]), jnp.maximum(ms[2], ms[3]))
                tot, val = None, None
                for n in range(4):
                    w = jnp.exp(ms[n] - top)
                    t = l[n, half, slot, rows] * w
                    v = acc[n, half, slot, rows] * w
                    tot, val = (t, v) if n == 0 else (tot + t, val + v)
                take_values(half, h, val)
                st = jnp.where(lane == k, top, st)
                st = jnp.where(lane == 4 + k, jnp.sum(tot, axis=1, keepdims=True), st)
        return st

    def p_copy(i):
        return rcopy(psend.at[i], precv.at[i], pts.at[i], ptr.at[i], (at(z, x + i_dx(i), c)))

    def s_copy(i):
        return rcopy(ssend.at[i], srecv.at[i], sts.at[i], str_.at[i], (at(z, x + i_dx(i), c)))

    def i_dx(i):
        return jnp.where(i == 0, 2, jnp.where(i == 1, 1, 3))

    def wu_spread(k):
        for i in range(3):
            wu_x(k, i, x).start()

    def wu_finish(k):
        for i in range(3):
            wu_x(k, i, from_x(i)).wait_recv()
        wu_hand(k, c).start()

    def kv_arrive(s):
        ring_step(kv_ring, s, lambda k: kv_hand(k, c).start())

    def wu_arrive(s, spread):
        ring_step(wu_ring, s, lambda k: None)
        for k in spread:
            wu_spread(k)

    def all_slots(chunk, masked, first):
        pair = pairs[chunk]

        def body(slot, carry):
            if masked:
                piece(chunk, pair, slot, True)
            else:
                seen = pair < own
                pl.when(seen)(lambda: piece(chunk, pair, slot, False))
                pl.when(jnp.logical_not(seen))(lambda: unseen(chunk, slot))
            pl.when(slot == 0)(first)
            return carry

        lax.fori_loop(0, NX, body, 0)

    kv_arrive(1)
    for k in (0,) + ks(1):
        kv_hand(k, 1 - c).wait_recv()
    all_slots(0, True, lambda: wu_arrive(1, ks(1)))
    for i in range(3):
        wg_x(i, from_x(i)).wait_recv()
    wg_hand(0, c).start()

    kv_arrive(2)
    for k in ks(2):
        kv_hand(k, 1 - c).wait_recv()
    all_slots(1, False, lambda: wu_arrive(2, (2,)))

    wu_finish(0)
    kv_arrive(3)
    for k in ks(3):
        kv_hand(k, 1 - c).wait_recv()

    def last(idx, carry):
        final = jnp.logical_and(idx >= 3, idx != 6)
        i = jnp.where(idx < 3, idx, jnp.where(idx < 6, idx - 3, 3))
        slot = lax.rem(x + jnp.where(i == 3, 0, i_dx(i)), NX)
        chunk = jnp.where(final, 3, 2)
        pair = jnp.where(final, pairs[3], pairs[2])

        @pl.when(idx == 3)
        def _():
            kv_arrive(4)
            for k in ks(4):
                kv_hand(k, 1 - c).wait_recv()

        seen = pair < own
        pl.when(seen)(lambda: piece(chunk, pair, slot, False))
        pl.when(jnp.logical_not(seen))(lambda: unseen(chunk, slot))

        @pl.when(jnp.logical_and(final, i < 3))
        def _():
            def put(half, h, val):
                col = (half * 2 + h) * 128
                psend[i, :, col : col + 128] = val.astype(bf16)

            st = jnp.concatenate((join(slot, put), jnp.zeros((64, 128), f32)), axis=0)
            ssend[i] = st.T[0:8]
            p_copy(i).start()
            s_copy(i).start()

        @pl.when(idx == 0)
        def _():
            wu_arrive(3, (5,))
            for ring in wg_rings:
                ring_start(ring)

        @pl.when(idx == 2)
        def _():
            for k in ks(1):
                wu_finish(k)

        @pl.when(idx == 3)
        def _():
            wu_arrive(4, ())
            wg_step(0, 1)

        for j in (1, 2, 3):
            @pl.when(idx == 3 + j)
            def _():
                wg_step(j, 1)

        @pl.when(idx == 7)
        def _():
            wg_step(0, 2)

        return carry

    lax.fori_loop(0, 8, last, 0)
    wg_step(1, 2)
    for i in range(3):
        ow_y(i, from_y(i)).wait_recv()
        ow_hand(i, c).start()

    def take(i):
        p_copy(i).wait_recv()
        s_copy(i).wait_recv()
        st = jnp.concatenate((srecv[i], jnp.zeros((120, 256), f32)), axis=0).T[0:ROWS]
        return st

    mine = {}

    def keep(half, h, val):
        mine[half, h] = val

    stats = [join(x, keep)] + [take(i) for i in range(3)]
    for k in (3, 6, 7):
        wu_spread(k)
    for h in range(2):
        parts = []
        for half in range(2):
            k = half * 2 + h
            col = k * 128
            ms = [st[:, k : k + 1] for st in stats]
            ls = [st[:, 4 + k : 5 + k] for st in stats]
            top = functools.reduce(jnp.maximum, ms)
            ws = [jnp.exp(a - top) for a in ms]
            tot = sum(w * t for w, t in zip(ws, ls))
            joined = mine[half, h] * ws[0]
            for i in range(3):
                joined = joined + precv[i, :, col : col + 128].astype(f32) * ws[i + 1]
            parts.append(joined / tot)
        diff = parts[0] - lam[h] * parts[1]
        heads[y, :, h * 128 : (h + 1) * 128] = rms_scale(diff, gain[...]).astype(bf16)

    for i in range(3):
        heads_y(i, y).start()

    wg_step(2, 2)
    wu_finish(2)
    wg_step(3, 2)
    wg_step(0, 3)
    wg_step(1, 3)

    loads[8].wait()
    loads[9].wait()
    for i in range(3):
        ow_hand(i, 1 - c).wait_recv()
    for i in range(3):
        heads_y(i, from_y(i)).wait_recv()
    width = stream.shape[2]
    for n in range(0, width, 512):
        cols = slice(n, n + 512)
        total = res[:, cols].astype(f32)
        for yy in range(NY):
            total = total + jnp.dot(heads[yy], ow[yy, :, cols], preferred_element_type=f32)
        stream[:, :, cols] = total.reshape(NY, ROWS // NY, 512)
    rows = stream[...].reshape(ROWS, width)
    normed = rms_scale(rows, mix_gain[...]).astype(bf16)
    for zz in range(NZ):
        ffn[zz] = normed[:, zz * 256 : (zz + 1) * 256]

    ff = hidden.shape[1]
    order = (0,) + ks(1) + ks(2) + ks(3) + ks(4)
    for n, k in enumerate(order):
        if n == 0:
            wu_finish(5)
            wg_step(2, 3)
        if n == 1:
            wg_step(3, 3)
        if n == 2:
            wu_finish(3)
            wg_step(0, 4)
        if n == 3:
            wg_step(1, 4)
        if n == 4:
            wu_finish(6)
            wg_step(2, 4)
        if n == 5:
            wg_step(3, 4)
            wu_finish(7)
        wg_hand(k, 1 - c).wait_recv()
        wu_hand(k, 1 - c).wait_recv()
        blk = hand_blk(k)
        rows_in = ffn[blk]
        if n == 7:
            for e, (w, pad) in enumerate(((wg, gate_pad), (wu, up_pad))):
                tip = jnp.dot(
                    rows_in[ROWS - 16 :], w[blk].reshape(256, ff), preferred_element_type=f32
                )
                tip = (tip[8:] + pad[ROWS : 8 + ROWS, :]).astype(bf16).astype(f32)
                edge_out[e] = tip[6:8]
            edge_copy().start()
        for w, pad in ((wg, gate_pad), (wu, up_pad)):
            pre = jnp.dot(rows_in, w[blk].reshape(256, ff), preferred_element_type=f32)
            if n > 0:
                pre = pre + pad[8 : 8 + ROWS, :]
            if n == 7:
                pre = pre.astype(bf16).astype(f32)
            pad[8 : 8 + ROWS, :] = pre

    def mix(top, size):
        for n in range(0, ff, 128):
            cols = slice(n, n + 128)
            conv = []
            for pad, taps in ((gate_pad, gate_taps), (up_pad, up_taps)):
                v = taps[0:1, cols] * pad[6 + top : 6 + top + size, cols]
                v = v + taps[1:2, cols] * pad[7 + top : 7 + top + size, cols]
                v = v + taps[2:3, cols] * pad[8 + top : 8 + top + size, cols]
                conv.append(v)
            hidden[top : top + size, cols] = (jax.nn.silu(conv[0]) * conv[1]).astype(bf16)

    mix(16, ROWS - 16)
    edge_copy().wait_recv()
    gate_pad[6:8, :] = jnp.where(r == 0, 0.0, edge_in[0])
    up_pad[6:8, :] = jnp.where(r == 0, 0.0, edge_in[1])
    mix(0, 16)

    for n in range(NY):
        cols = slice(n * 512, (n + 1) * 512)
        down = jnp.dot(hidden[...], dw[:, cols], preferred_element_type=f32)
        part[n] = down.astype(bf16).reshape(NY, ROWS // NY, 512)
        for i in range(3):
            down_y(i, n).start()
    edge_copy().wait_send()
    for i in range(3):
        q_copy(i, x).wait_send()
        wg_x(i, x).wait_send()
        p_copy(i).wait_send()
        s_copy(i).wait_send()
        ow_y(i, y).wait_send()
        ow_hand(i, c).wait_send()
        heads_y(i, y).wait_send()
    for ring in [kv_ring, wu_ring] + wg_rings:
        for s in range(1, 5):
            only(plus_n, s, lambda: ring[0](s).wait_send())
            only(minus_n, s, lambda: ring[1](s).wait_send())
    for k in range(8):
        kv_hand(k, c).wait_send()
        wg_hand(k, c).wait_send()
        wu_hand(k, c).wait_send()
        for i in range(3):
            wu_x(k, i, x).wait_send()
    for n in range(NY):
        cols = slice(n * 512, (n + 1) * 512)
        total = stream[y, :, cols] + part[n, y].astype(f32)
        for i in range(3):
            down_y(i, n).wait_recv()
            total = total + drecv[i, n].astype(f32)
        out[:, cols] = total.astype(bf16)
    for i in range(3):
        for n in range(NY):
            down_y(i, n).wait_send()


def layer(*args):
    ANY = pl.BlockSpec(memory_space=pl.ANY)
    VM = pl.BlockSpec(memory_space=pltpu.VMEM)
    SM = pl.BlockSpec(memory_space=pltpu.SMEM)
    ff, width = args[5].shape[1], args[8].shape[1]
    dma = pltpu.SemaphoreType.DMA
    sems = [(10,), (2, 3), (2, 4), (2, 4), (8,), (8,), (2, 4), (2, 4), (8, 3), (8, 3), (8,), (8,)]
    sems += [(3,), (3,), (NX, 2, 4), (NX, 2, 4), (8,), (8,), (3,), (3,), (3,), (3,)]
    sems += [(3,), (3,), (3,), (3,), (3,), (3,), None, None, (3, 4), (3, 4)]
    return pl.pallas_call(
        layer_kernel,
        out_shape=jax.ShapeDtypeStruct((ROWS // NY, width), bf16),
        in_specs=[ANY] * 10 + [SM] + [VM] * 4,
        out_specs=VM,
        scratch_shapes=[
            pltpu.VMEM((4, ROWS, 256), bf16),
            pltpu.VMEM((8, 2, ROWS, 512), bf16),
            pltpu.VMEM((8, 4, 2, 32, ff), bf16),
            pltpu.VMEM((8, 4, 2, 32, ff), bf16),
            pltpu.VMEM((2, 4, 2 * ROWS, 128), bf16),
            pltpu.VMEM((4, 2, 4, 2 * ROWS, 128), f32),
            pltpu.VMEM((4, 2, 4, 2 * ROWS, 128), f32),
            pltpu.VMEM((4, 2, 4, 2 * ROWS, 128), f32),
            pltpu.VMEM((3, ROWS, 512), bf16),
            pltpu.VMEM((3, ROWS, 512), bf16),
            pltpu.VMEM((3, 8, 256), f32),
            pltpu.VMEM((3, 8, 256), f32),
            pltpu.VMEM((NY, ROWS, 256), bf16),
            pltpu.VMEM((NY, 256, width), bf16),
            pltpu.VMEM((ff, width), bf16),
            pltpu.VMEM((ROWS, width), bf16),
            pltpu.VMEM((NY, ROWS // NY, width), f32),
            pltpu.VMEM((NZ, ROWS, 256), bf16),
            pltpu.VMEM((8 + ROWS, ff), f32),
            pltpu.VMEM((8 + ROWS, ff), f32),
            pltpu.VMEM((ROWS, ff), bf16),
            pltpu.VMEM((2, 2, ff), f32),
            pltpu.VMEM((2, 2, ff), f32),
            pltpu.VMEM((NY, NY, ROWS // NY, 512), bf16),
            pltpu.VMEM((3, NY, ROWS // NY, 512), bf16),
        ] + [dma if s is None else dma(s) for s in sems],
        compiler_params=pltpu.CompilerParams(
            collective_id=0, has_side_effects=True, vmem_limit_bytes=63 * 1024 * 1024
        ),
        name="layer",
    )(*args)


def shards(
    q_first, k_first, q_second, k_second, values, lambdas, head_gain, out_weight, residual_in,
    mix_gain, gate_weight, up_weight, gate_taps, up_taps, down_weight,
):
    return layer(
        q_first, q_second, k_first, k_second, values, gate_weight, up_weight, out_weight,
        residual_in, down_weight, lambdas, head_gain[None], mix_gain[None], gate_taps, up_taps,
    )


def solution(mesh):
    in_specs = (
        P("sp", "tp"), P("sp", "tp"), P("sp", "tp"), P("sp", "tp"), P("sp", "tp"),
        P("tp"), P(), P("tp", None), P("sp", None), P(),
        P("sp", "tp"), P("sp", "tp"), P(None, "tp"), P(None, "tp"), P("tp", None),
    )
    out_specs = P(("sp", "tp"), None)
    return jax.shard_map(shards, mesh=mesh, in_specs=in_specs, out_specs=out_specs, check_vma=False)
```

```python
import functools

import jax
import jax.numpy as jnp
from jax import lax
from jax.experimental import pallas as pl
from jax.experimental.pallas import tpu as pltpu
from jax.sharding import PartitionSpec as P

MESH = pl.DeviceIdType.MESH
norm_eps = 1e-06
ROWS = 192
NX, NZ, NY = 4, 8, 4
DX = (2, 1, 3)
HIDE = -2e30
FLOOR = -1e30
f32, bf16 = jnp.float32, jnp.bfloat16


def rms_scale(field, gain):
    return field * lax.rsqrt(jnp.mean(field * field, axis=-1, keepdims=True) + norm_eps) * gain


def layer_kernel(
    qa, qb, ka, kb, va, gw, uw, out_w, res_in, down_w, lam, gain, mix_gain, gate_taps, up_taps,
    out,
    q, kv, wg, wu, qz, m, l, acc, psend, precv, ssend, srecv,
    heads, ow, dw, res, stream, ffn, pad, hidden, edge_out, edge_in, part, drecv,
    loc, snd, one, hsr, kvr, kdr, wur, wxr, wdr, gzr, gdr, dyr,
):
    r = lax.axis_index("sp")
    y = lax.axis_index("tp")
    z, x, c = r // 8, (r // 2) % 4, r % 2

    def at(zz, xx, cc):
        return (lax.rem(zz + NZ, NZ) * 8 + lax.rem(xx + NX, NX) * 2 + cc, y)

    mate = (r + 1 - 2 * c, y)
    up_dev, down_dev = at(z + 1, x, c), at(z - 1, x, c)

    def rcopy(src, dst, ss, rs, dev):
        return pltpu.make_async_remote_copy(
            src_ref=src, dst_ref=dst, send_sem=ss, recv_sem=rs, device_id=dev, device_id_type=MESH
        )

    cut, ff = wg.shape[4], hidden.shape[1]
    loads = [
        (qa, q.at[x, :, 0:128]),
        (qb, q.at[x, :, 128:256]),
        (ka, kv.at[z, c, :, 0:128]),
        (kb, kv.at[z, c, :, 128:256]),
        (va, kv.at[z, c, :, 256:512]),
        (gw.at[:, 0:cut], wg.at[z, x, c]),
        (gw.at[:, cut:ff], wu.at[z, x, c, :, 0 : ff - cut]),
        (uw, wu.at[z, x, c, :, ff - cut : 2 * ff - cut]),
        (out_w, ow.at[y]),
        (res_in, res),
        (down_w, dw),
    ]
    loads = [pltpu.make_async_copy(s, d, loc.at[i]) for i, (s, d) in enumerate(loads)]
    for d in loads:
        d.start()
    barrier = pltpu.get_barrier_semaphore()
    across = [(r, lax.rem(y + d, NY)) for d in DX]
    after, before = (lax.rem(r + 1, 64), y), (lax.rem(r + 63, 64), y)
    greeted = [up_dev, down_dev, mate, after, before] + [at(z, x + d, c) for d in DX] + across
    for dev in greeted:
        pl.semaphore_signal(barrier, inc=1, device_id=dev, device_id_type=MESH)
    pl.semaphore_wait(barrier, len(greeted))
    for d in loads[:5]:
        d.wait()

    def q_copy(i, slot):
        return rcopy(q.at[slot], q.at[slot], snd.at[0], one.at[0], at(z, x + DX[i], c))

    plus_n, minus_n = 4 - c, 3 + c

    def z_ring(ref_at, sends, recvs):
        def plus(s):
            blk = lax.rem(z - s + 1 + NZ, NZ)
            return rcopy(ref_at(blk), ref_at(blk), sends, recvs.at[0, s - 1], up_dev)

        def minus(s):
            blk = lax.rem(z + s - 1, NZ)
            return rcopy(ref_at(blk), ref_at(blk), sends, recvs.at[1, s - 1], down_dev)

        def plus_in(s):
            blk = lax.rem(z - s + NZ, NZ)
            return rcopy(ref_at(blk), ref_at(blk), sends, recvs.at[0, s - 1], up_dev)

        def minus_in(s):
            blk = lax.rem(z + s, NZ)
            return rcopy(ref_at(blk), ref_at(blk), sends, recvs.at[1, s - 1], down_dev)

        return plus, minus, plus_in, minus_in

    def only(n, s, fn):
        if s <= 3:
            fn()
        elif s == 4:
            pl.when(n == 4)(fn)

    kv_rings = [
        z_ring(lambda b, h=h: kv.at[b, c, h * 96 : (h + 1) * 96], snd.at[1], kvr.at[h])
        for h in range(2)
    ]
    wu_ring = z_ring(lambda b: wu.at[b, x, c], snd.at[2], wur)
    wg_rings = [
        z_ring(lambda b, j=j: wg.at[b, lax.rem(x + j, NX), c], snd.at[3], gzr.at[j])
        for j in range(NX)
    ]

    def wg_step(j, s):
        ring_step(wg_rings[j], s, lambda k: None)
        if j == NX - 1:
            for k in ks(s):
                wg_hand(k, c).start()


    def hand_blk(k):
        off = (0, -1, -2, -3, 1, 2, 3, 4)[k]
        return lax.rem(z + off + NZ, NZ)

    def kv_hand(k, lane):
        b = hand_blk(k)
        return rcopy(kv.at[b, lane], kv.at[b, lane], snd.at[4], kdr.at[k], mate)

    def wg_hand(k, lane):
        b = hand_blk(k)
        return rcopy(wg.at[b, :, lane], wg.at[b, :, lane], snd.at[5], gdr.at[k], mate)

    def wu_hand(k, lane):
        b = hand_blk(k)
        return rcopy(wu.at[b, :, lane], wu.at[b, :, lane], snd.at[6], wdr.at[k], mate)

    toward = 1 - 2 * c

    def wu_x(k, d):
        ref = wu.at[hand_blk(k), x, c]
        return rcopy(ref, ref, snd.at[7], wxr.at[k, 0], at(z, x + d, c))

    def wu_x2(k):
        ref = wu.at[hand_blk(k), lax.rem(x - toward + NX, NX), c]
        return rcopy(ref, ref, snd.at[8], wxr.at[k, 1], at(z, x + toward, c))

    def wg_x(i, xx):
        return rcopy(wg.at[z, xx, c], wg.at[z, xx, c], snd.at[9], one.at[1], at(z, x + DX[i], c))

    def got(ref, sem):
        rcopy(ref, ref, snd.at[0], sem, mate).wait_recv()

    def gone(ref, n):
        rcopy(ref, ref, snd.at[n], one.at[0], mate).wait_send()

    def from_x(i):
        return lax.rem(x - DX[i] + NX, NX)

    def ring_start(ring):
        ring[0](1).start()
        ring[1](1).start()

    def ring_step(ring, s, hand):
        def p():
            ring[2](s).wait_recv()
            only(plus_n, s + 1, lambda: ring[0](s + 1).start())
            if s < 4:
                hand(s)
            else:
                hand(7)

        def n():
            ring[3](s).wait_recv()
            only(minus_n, s + 1, lambda: ring[1](s + 1).start())
            if s < 4:
                hand(3 + s)
            else:
                hand(7)

        only(plus_n, s, p)
        only(minus_n, s, n)

    def ks(s):
        return (s, 3 + s) if s < 4 else (7,)

    def from_y(i):
        return lax.rem(y - DX[i] + NY, NY)

    half_cols = ow.shape[2] // 2

    def ow_y(i, yy):
        ref = ow.at[yy, :, pl.ds(pl.multiple_of(c * half_cols, 128), half_cols)]
        return rcopy(ref, ref, snd.at[10], one.at[2], across[i])

    def ow_hand(i, lane):
        ref = ow.at[from_y(i), :, pl.ds(pl.multiple_of(lane * half_cols, 128), half_cols)]
        return rcopy(ref, ref, snd.at[11], one.at[3], mate)

    def heads_y(i, yy):
        return rcopy(heads.at[yy], heads.at[yy], snd.at[12], hsr.at[i], across[i])

    def edge_copy():
        return rcopy(edge_out, edge_in, snd.at[13], one.at[5], after)

    def down_y(i, n):
        return rcopy(
            part.at[n, across[i][1]], drecv.at[i, n], snd.at[14], dyr.at[n], across[i]
        )

    for i in range(3):
        q_copy(i, x).start()
    ring_start(kv_rings[0])
    ring_start(kv_rings[1])
    kv_hand(0, c).start()
    for d in loads[5:9]:
        d.wait()
    for i in range(3):
        ow_y(i, y).start()
    ring_start(wu_ring)

    lane = lax.broadcasted_iota(jnp.int32, (ROWS, 128), 1)

    def prepare(slot):
        for half in range(2):
            block = q[slot, :, half * 128 : (half + 1) * 128] * bf16(0.125)
            zero = jnp.zeros_like(block)
            qz[half, slot, 0:ROWS] = jnp.where(lane < 64, block, zero)
            qz[half, slot, ROWS : 2 * ROWS] = jnp.where(lane < 64, zero, block)

    prepare(x)
    ring_step(kv_rings[0], 1, lambda k: None)
    for i in range(3):
        wg_x(i, x).start()
    wu_x(0, 1).start()
    wu_x(0, 3).start()
    ring_step(kv_rings[1], 1, lambda k: kv_hand(k, c).start())
    got(q.at[0:3], one.at[0])
    for i in range(3):
        prepare(from_x(i))

    def piece(chunk, pair, slot, masked):
        if masked:
            j = lax.broadcasted_iota(jnp.int32, (1, 768), 1)
            second = (j >= 384).astype(jnp.int32)
            core = ((j - 384 * second) >= 192).astype(jnp.int32)
            off = j - 384 * second - 192 * core
            key_pos = ((2 * pair + second) * 8 + x * 2 + core) * ROWS + off
            i = lax.broadcasted_iota(jnp.int32, (2 * ROWS, 1), 0)
            i = i - ROWS * (i >= ROWS).astype(jnp.int32)
            query_pos = (z * 8 + slot * 2 + c) * ROWS + i
            visible = key_pos <= query_pos
        for half in range(2):
            keys = kv[pl.ds(2 * pair, 2), :, :, half * 128 : (half + 1) * 128].reshape(768, 128)
            s = lax.dot_general(
                qz[half, slot], keys, (((1,), (1,)), ((), ())), preferred_element_type=f32
            )
            if masked:
                s = jnp.where(visible, s, HIDE)
            new = jnp.broadcast_to(
                jnp.maximum(jnp.max(s, axis=1, keepdims=True), FLOOR), (2 * ROWS, 128)
            )
            m[chunk, half, slot] = new
            e = jnp.exp(s - new[:, 0:1])
            part_sum = e[:, 0:128]
            for t in range(1, 6):
                part_sum = part_sum + e[:, t * 128 : (t + 1) * 128]
            l[chunk, half, slot] = part_sum
            eb = e.astype(bf16)
            for h in range(2):
                rows = slice(h * ROWS, (h + 1) * ROWS)
                vals = kv[pl.ds(2 * pair, 2), :, :, 256 + h * 128 : 384 + h * 128].reshape(768, 128)
                acc[chunk, half, slot, rows] = jnp.dot(eb[rows], vals, preferred_element_type=f32)

    def unseen(chunk, slot):
        for half in range(2):
            m[chunk, half, slot] = jnp.full((2 * ROWS, 128), FLOOR, f32)
            l[chunk, half, slot] = jnp.zeros((2 * ROWS, 128), f32)
            acc[chunk, half, slot] = jnp.zeros((2 * ROWS, 128), f32)

    own = z // 2
    odd = z % 2
    pairs = (
        own,
        lax.rem(own + jnp.where(odd == 1, 1, 3), 4),
        lax.rem(own + jnp.where(odd == 1, 3, 1), 4),
        lax.rem(own + 2, 4),
    )

    def join(slot, take_values):
        st = jnp.zeros((ROWS, 128), f32)
        for half in range(2):
            for h in range(2):
                rows = slice(h * ROWS, (h + 1) * ROWS)
                k = half * 2 + h
                ms = [m[n, half, slot, rows] for n in range(4)]
                top = jnp.maximum(jnp.maximum(ms[0], ms[1]), jnp.maximum(ms[2], ms[3]))
                tot, val = None, None
                for n in range(4):
                    w = jnp.exp(ms[n] - top)
                    t = l[n, half, slot, rows] * w
                    v = acc[n, half, slot, rows] * w
                    tot, val = (t, v) if n == 0 else (tot + t, val + v)
                take_values(half, h, val)
                st = jnp.where(lane == k, top, st)
                st = jnp.where(lane == 4 + k, jnp.sum(tot, axis=1, keepdims=True), st)
        return st

    def p_copy(i):
        return rcopy(psend.at[i], precv.at[i], snd.at[15], one.at[6], (at(z, x + i_dx(i), c)))

    def s_copy(i):
        return rcopy(ssend.at[i], srecv.at[i], snd.at[16], one.at[7], (at(z, x + i_dx(i), c)))

    def i_dx(i):
        return jnp.where(i == 0, 2, jnp.where(i == 1, 1, 3))

    def wu_spread(k):
        wu_x(k, 1).start()
        wu_x(k, 3).start()

    def wu_mid(k):
        got(wu.at[0, 0:2, c], wxr.at[k, 0])
        wu_x2(k).start()

    def wu_finish(k):
        got(wu.at[0, 0, c], wxr.at[k, 1])
        wu_hand(k, c).start()

    def kv_arrive(s, h):
        ring_step(kv_rings[h], s, lambda k: kv_hand(k, c).start() if h == 1 else None)

    def wu_arrive(s, spread):
        ring_step(wu_ring, s, lambda k: None)
        for k in spread:
            wu_spread(k)

    def all_slots(chunk, masked, first, s):
        pair = pairs[chunk]

        def body(slot, carry):
            if masked:
                piece(chunk, pair, slot, True)
            else:
                seen = pair < own
                pl.when(seen)(lambda: piece(chunk, pair, slot, False))
                pl.when(jnp.logical_not(seen))(lambda: unseen(chunk, slot))
            pl.when(slot == 0)(first)
            pl.when(slot == 1)(lambda: kv_arrive(s, 0))
            pl.when(slot == (3 if masked else 2))(lambda: kv_arrive(s, 1))
            return carry

        lax.fori_loop(0, NX, body, 0)

    for k in (0,) + ks(1):
        kv_hand(k, 1 - c).wait_recv()
    all_slots(0, True, lambda: wu_arrive(1, ks(1)), 2)
    got(wg.at[0, 0:3, c], one.at[1])
    wg_hand(0, c).start()
    wu_mid(0)
    for k in ks(2):
        kv_hand(k, 1 - c).wait_recv()
    all_slots(1, False, lambda: wu_arrive(2, ks(2)), 3)
    for k in ks(3):
        kv_hand(k, 1 - c).wait_recv()

    def last(idx, carry):
        final = jnp.logical_and(idx >= 3, idx != 6)
        i = jnp.where(idx < 3, idx, jnp.where(idx < 6, idx - 3, 3))
        slot = lax.rem(x + jnp.where(i == 3, 0, i_dx(i)), NX)
        chunk = jnp.where(final, 3, 2)
        pair = jnp.where(final, pairs[3], pairs[2])

        @pl.when(idx == 3)
        def _():
            for k in ks(4):
                kv_hand(k, 1 - c).wait_recv()

        seen = pair < own
        pl.when(seen)(lambda: piece(chunk, pair, slot, False))
        pl.when(jnp.logical_not(seen))(lambda: unseen(chunk, slot))

        @pl.when(jnp.logical_and(final, i < 3))
        def _():
            def put(half, h, val):
                col = (half * 2 + h) * 128
                psend[i, :, col : col + 128] = val.astype(bf16)

            st = jnp.concatenate((join(slot, put), jnp.zeros((64, 128), f32)), axis=0)
            ssend[i] = st.T[0:8]
            p_copy(i).start()
            s_copy(i).start()

        @pl.when(idx == 0)
        def _():
            wu_arrive(3, ())
            for ring in wg_rings:
                ring_start(ring)

        @pl.when(idx == 1)
        def _():
            wu_finish(0)
            for k in ks(1):
                wu_mid(k)

        @pl.when(idx == 2)
        def _():
            kv_arrive(4, 0)
            kv_arrive(4, 1)

        @pl.when(idx == 3)
        def _():
            wu_arrive(4, ())
            wg_step(0, 1)

        for j in (1, 2, 3):
            @pl.when(idx == 3 + j)
            def _():
                wg_step(j, 1)

        @pl.when(idx == 5)
        def _():
            for k in ks(1):
                wu_finish(k)

        @pl.when(idx == 7)
        def _():
            wg_step(0, 2)
            for k in ks(2):
                wu_mid(k)

        return carry

    lax.fori_loop(0, 8, last, 0)
    for k in (3, 6, 7):
        wu_spread(k)
    wg_step(1, 2)
    wg_step(2, 2)
    wg_step(3, 2)
    got(ow.at[0:3, :, 0:half_cols], one.at[2])
    for i in range(3):
        ow_hand(i, c).start()

    def take(i):
        st = jnp.concatenate((srecv[i], jnp.zeros((120, 256), f32)), axis=0).T[0:ROWS]
        return st

    mine = {}

    def keep(half, h, val):
        mine[half, h] = val

    stats = [join(x, keep)]
    got(precv, one.at[6])
    got(srecv, one.at[7])
    stats += [take(i) for i in range(3)]
    for h in range(2):
        parts = []
        for half in range(2):
            k = half * 2 + h
            col = k * 128
            ms = [st[:, k : k + 1] for st in stats]
            ls = [st[:, 4 + k : 5 + k] for st in stats]
            top = functools.reduce(jnp.maximum, ms)
            ws = [jnp.exp(a - top) for a in ms]
            tot = sum(w * t for w, t in zip(ws, ls))
            joined = mine[half, h] * ws[0]
            for i in range(3):
                joined = joined + precv[i, :, col : col + 128].astype(f32) * ws[i + 1]
            parts.append(joined / tot)
        diff = parts[0] - lam[h] * parts[1]
        heads[y, :, h * 128 : (h + 1) * 128] = rms_scale(diff, gain[...]).astype(bf16)

    for i in range(3):
        heads_y(i, y).start()

    wg_step(0, 3)
    for k in ks(2):
        wu_finish(k)
    wg_step(1, 3)
    wu_mid(3)
    wg_step(2, 3)
    wg_step(3, 3)
    wu_mid(6)

    loads[9].wait()
    loads[10].wait()
    got(ow.at[0:3, :, 0:half_cols], one.at[3])
    width = stream.shape[2]
    for i in (None, 1, 2, 0):
        yy = y
        if i is not None:
            yy = from_y(i)
            heads_y(i, yy).wait_recv()
        for n in range(0, width, 512):
            cols = slice(n, n + 512)
            more = jnp.dot(heads[yy], ow[yy, :, cols], preferred_element_type=f32)
            more = more.reshape(NY, ROWS // NY, 512)
            if i is None:
                more = more + res[:, cols].astype(f32).reshape(NY, ROWS // NY, 512)
            else:
                more = more + stream[:, :, cols]
            stream[:, :, cols] = more
    rows = stream[...].reshape(ROWS, width)
    normed = rms_scale(rows, mix_gain[...]).astype(bf16)
    for zz in range(NZ):
        ffn[zz] = normed[:, zz * 256 : (zz + 1) * 256]

    order = (0,) + ks(1) + ks(2) + ks(3) + ks(4)
    pieces = ((wg, slice(0, cut)), (wu, slice(cut, 2 * ff)))
    for n in range(0, 8, 2):
        two = order[n : n + 2]
        if n == 0:
            wg_step(0, 4)
            wu_mid(7)
        if n == 2:
            wg_step(1, 4)
            wg_step(2, 4)
            wu_finish(3)
        if n == 4:
            wu_finish(6)
            wg_step(3, 4)
            wu_finish(7)
        for k in two:
            wg_hand(k, 1 - c).wait_recv()
            wu_hand(k, 1 - c).wait_recv()
        blks = [hand_blk(k) for k in two]

        def product(w, top):
            return sum(
                jnp.dot(ffn[b, top:], w[b].reshape(256, -1), preferred_element_type=f32)
                for b in blks
            )

        if n == 6:
            for w, cols in pieces:
                tip = product(w, ROWS - 16)
                tip = (tip[8:] + pad[ROWS : 8 + ROWS, cols]).astype(bf16).astype(f32)
                edge_out[:, cols] = tip[6:8]
            edge_copy().start()
        for w, cols in pieces:
            pre = product(w, 0)
            if n > 0:
                pre = pre + pad[8 : 8 + ROWS, cols]
            if n == 6:
                pre = pre.astype(bf16).astype(f32)
            pad[8 : 8 + ROWS, cols] = pre

    def mix(top, size):
        for n in range(0, ff, 128):
            cols = slice(n, n + 128)
            conv = []
            for base, taps in ((0, gate_taps), (ff, up_taps)):
                there = slice(base + n, base + n + 128)
                v = taps[0:1, cols] * pad[6 + top : 6 + top + size, there]
                v = v + taps[1:2, cols] * pad[7 + top : 7 + top + size, there]
                v = v + taps[2:3, cols] * pad[8 + top : 8 + top + size, there]
                conv.append(v)
            hidden[top : top + size, cols] = (jax.nn.silu(conv[0]) * conv[1]).astype(bf16)

    mix(16, ROWS - 16)
    edge_copy().wait_recv()
    pad[6:8, :] = jnp.where(r == 0, 0.0, edge_in[...])
    mix(0, 16)

    for n in range(NY):
        cols = slice(n * 512, (n + 1) * 512)
        down = jnp.dot(hidden[...], dw[:, cols], preferred_element_type=f32)
        part[n] = down.astype(bf16).reshape(NY, ROWS // NY, 512)
        for i in range(3):
            down_y(i, n).start()
    edge_copy().wait_send()
    gone(q.at[0:3], 0)
    gone(kv.at[0:7, 0], 1)
    gone(wu.at[0:7, 0, 0], 2)
    gone(wg.at[0:7, :, 0], 3)
    gone(kv.at[:, 0], 4)
    gone(wg.at[:, :, 0], 5)
    gone(wu.at[:, :, 0], 6)
    gone(wu.at[:, 0:2, 0], 7)
    gone(wu.at[:, 0, 0], 8)
    gone(wg.at[0, 0:3, 0], 9)
    gone(ow.at[0:3, :, 0:half_cols], 10)
    gone(ow.at[0:3, :, 0:half_cols], 11)
    gone(heads.at[0:3], 12)
    gone(psend, 15)
    gone(ssend, 16)
    for n in range(NY):
        cols = slice(n * 512, (n + 1) * 512)
        total = stream[y, :, cols] + part[n, y].astype(f32)
        got(drecv.at[:, n], dyr.at[n])
        for i in range(3):
            total = total + drecv[i, n].astype(f32)
        out[:, cols] = total.astype(bf16)
    gone(drecv, 14)


def layer(*args):
    ANY = pl.BlockSpec(memory_space=pl.ANY)
    VM = pl.BlockSpec(memory_space=pltpu.VMEM)
    SM = pl.BlockSpec(memory_space=pltpu.SMEM)
    ff, width = args[5].shape[1], args[8].shape[1]
    dma = pltpu.SemaphoreType.DMA
    cut = 9 * 128 if ff > 9 * 128 else ff // 2
    sems = [(11,), (17,), (8,), (3,), (2, 2, 4), (8,), (2, 4), (8, 2), (8,), (NX, 2, 4), (8,), (NY,)]
    return pl.pallas_call(
        layer_kernel,
        out_shape=jax.ShapeDtypeStruct((ROWS // NY, width), bf16),
        in_specs=[ANY] * 10 + [SM] + [VM] * 4,
        out_specs=VM,
        scratch_shapes=[
            pltpu.VMEM((4, ROWS, 256), bf16),
            pltpu.VMEM((8, 2, ROWS, 512), bf16),
            pltpu.VMEM((8, 4, 2, 32, cut), bf16),
            pltpu.VMEM((8, 4, 2, 32, 2 * ff - cut), bf16),
            pltpu.VMEM((2, 4, 2 * ROWS, 128), bf16),
            pltpu.VMEM((4, 2, 4, 2 * ROWS, 128), f32),
            pltpu.VMEM((4, 2, 4, 2 * ROWS, 128), f32),
            pltpu.VMEM((4, 2, 4, 2 * ROWS, 128), f32),
            pltpu.VMEM((3, ROWS, 512), bf16),
            pltpu.VMEM((3, ROWS, 512), bf16),
            pltpu.VMEM((3, 8, 256), f32),
            pltpu.VMEM((3, 8, 256), f32),
            pltpu.VMEM((NY, ROWS, 256), bf16),
            pltpu.VMEM((NY, 256, width), bf16),
            pltpu.VMEM((ff, width), bf16),
            pltpu.VMEM((ROWS, width), bf16),
            pltpu.VMEM((NY, ROWS // NY, width), f32),
            pltpu.VMEM((NZ, ROWS, 256), bf16),
            pltpu.VMEM((8 + ROWS, 2 * ff), f32),
            pltpu.VMEM((ROWS, ff), bf16),
            pltpu.VMEM((2, 2 * ff), f32),
            pltpu.VMEM((2, 2 * ff), f32),
            pltpu.VMEM((NY, NY, ROWS // NY, 512), bf16),
            pltpu.VMEM((3, NY, ROWS // NY, 512), bf16),
        ] + [dma(s) for s in sems],
        compiler_params=pltpu.CompilerParams(
            collective_id=0, has_side_effects=True, vmem_limit_bytes=63 * 1024 * 1024
        ),
        name="layer",
    )(*args)


def shards(
    q_first, k_first, q_second, k_second, values, lambdas, head_gain, out_weight, residual_in,
    mix_gain, gate_weight, up_weight, gate_taps, up_taps, down_weight,
):
    return layer(
        q_first, q_second, k_first, k_second, values, gate_weight, up_weight, out_weight,
        residual_in, down_weight, lambdas, head_gain[None], mix_gain[None], gate_taps, up_taps,
    )


def solution(mesh):
    in_specs = (
        P("sp", "tp"), P("sp", "tp"), P("sp", "tp"), P("sp", "tp"), P("sp", "tp"),
        P("tp"), P(), P("tp", None), P("sp", None), P(),
        P("sp", "tp"), P("sp", "tp"), P(None, "tp"), P(None, "tp"), P("tp", None),
    )
    out_specs = P(("sp", "tp"), None)
    return jax.shard_map(shards, mesh=mesh, in_specs=in_specs, out_specs=out_specs, check_vma=False)
```

```python
import functools

import jax
import jax.numpy as jnp
from jax import lax
from jax.experimental import pallas as pl
from jax.experimental.pallas import tpu as pltpu
from jax.sharding import PartitionSpec as P

MESH = pl.DeviceIdType.MESH
norm_eps = 1e-06
ROWS = 192
NX, NZ, NY = 4, 8, 4
DX = (2, 1, 3)
HIDE = -2e30
FLOOR = -1e30
f32, bf16 = jnp.float32, jnp.bfloat16


def rms_scale(field, gain):
    return field * lax.rsqrt(jnp.mean(field * field, axis=-1, keepdims=True) + norm_eps) * gain


def layer_kernel(
    qa, qb, ka, kb, va, gw, uw, out_w, res_in, down_w, lam, gain, mix_gain, gate_taps, up_taps,
    out,
    q, kv, wg, wu, qz, m, l, acc, psend, precv, ssend, srecv,
    heads, ow, dw, res, stream, ffn, pad, hidden, edge_out, edge_in, part, drecv,
    loc, snd, one, hsr, kvr, kdr, wur, wxr, wdr, gzr, gdr, dyr,
):
    r = lax.axis_index("sp")
    y = lax.axis_index("tp")
    z, x, c = r // 8, (r // 2) % 4, r % 2

    def at(zz, xx, cc):
        return (lax.rem(zz + NZ, NZ) * 8 + lax.rem(xx + NX, NX) * 2 + cc, y)

    mate = (r + 1 - 2 * c, y)
    up_dev, down_dev = at(z + 1, x, c), at(z - 1, x, c)

    def rcopy(src, dst, ss, rs, dev):
        return pltpu.make_async_remote_copy(
            src_ref=src, dst_ref=dst, send_sem=ss, recv_sem=rs, device_id=dev, device_id_type=MESH
        )

    cut, ff = wg.shape[4], hidden.shape[1]
    loads = [
        (qa, q.at[x, :, 0:128]),
        (qb, q.at[x, :, 128:256]),
        (ka, kv.at[z, c, :, 0:128]),
        (kb, kv.at[z, c, :, 128:256]),
        (va, kv.at[z, c, :, 256:512]),
        (gw.at[:, 0:cut], wg.at[z, x, c]),
        (gw.at[:, cut:ff], wu.at[z, x, c, :, 0 : ff - cut]),
        (uw, wu.at[z, x, c, :, ff - cut : 2 * ff - cut]),
        (out_w, ow.at[y]),
        (res_in, res),
        (down_w, dw),
    ]
    loads = [pltpu.make_async_copy(s, d, loc.at[i]) for i, (s, d) in enumerate(loads)]
    for d in loads:
        d.start()
    barrier = pltpu.get_barrier_semaphore()
    across = [(r, lax.rem(y + d, NY)) for d in DX]
    after, before = (lax.rem(r + 1, 64), y), (lax.rem(r + 63, 64), y)
    greeted = [up_dev, down_dev, mate, after, before] + [at(z, x + d, c) for d in DX] + across
    for dev in greeted:
        pl.semaphore_signal(barrier, inc=1, device_id=dev, device_id_type=MESH)
    pl.semaphore_wait(barrier, len(greeted))
    for d in loads[:5]:
        d.wait()

    def q_copy(i, slot):
        return rcopy(q.at[slot], q.at[slot], snd.at[0], one.at[0], at(z, x + DX[i], c))

    plus_n, minus_n = 4 - c, 3 + c

    def z_ring(ref_at, sends, recvs):
        def plus(s):
            blk = lax.rem(z - s + 1 + NZ, NZ)
            return rcopy(ref_at(blk), ref_at(blk), sends, recvs.at[0, s - 1], up_dev)

        def minus(s):
            blk = lax.rem(z + s - 1, NZ)
            return rcopy(ref_at(blk), ref_at(blk), sends, recvs.at[1, s - 1], down_dev)

        def plus_in(s):
            blk = lax.rem(z - s + NZ, NZ)
            return rcopy(ref_at(blk), ref_at(blk), sends, recvs.at[0, s - 1], up_dev)

        def minus_in(s):
            blk = lax.rem(z + s, NZ)
            return rcopy(ref_at(blk), ref_at(blk), sends, recvs.at[1, s - 1], down_dev)

        return plus, minus, plus_in, minus_in

    def only(n, s, fn):
        if s <= 3:
            fn()
        elif s == 4:
            pl.when(n == 4)(fn)

    kv_rings = [
        z_ring(lambda b, h=h: kv.at[b, c, h * 96 : (h + 1) * 96], snd.at[1], kvr.at[h])
        for h in range(2)
    ]
    wu_ring = z_ring(lambda b: wu.at[b, x, c], snd.at[2], wur)
    wg_rings = [
        z_ring(lambda b, j=j: wg.at[b, lax.rem(x + j, NX), c], snd.at[3], gzr.at[j])
        for j in range(NX)
    ]

    def wg_step(j, s):
        ring_step(wg_rings[j], s, lambda k: None)
        if j == NX - 1:
            for k in ks(s):
                wg_hand(k, c).start()


    def hand_blk(k):
        off = (0, -1, -2, -3, 1, 2, 3, 4)[k]
        return lax.rem(z + off + NZ, NZ)

    def kv_hand(k, lane):
        b = hand_blk(k)
        return rcopy(kv.at[b, lane], kv.at[b, lane], snd.at[4], kdr.at[k], mate)

    def wg_hand(k, lane):
        b = hand_blk(k)
        return rcopy(wg.at[b, :, lane], wg.at[b, :, lane], snd.at[5], gdr.at[k], mate)

    def wu_hand(k, lane):
        b = hand_blk(k)
        return rcopy(wu.at[b, :, lane], wu.at[b, :, lane], snd.at[6], wdr.at[k], mate)

    toward = 1 - 2 * c

    def wu_x(k, d):
        ref = wu.at[hand_blk(k), x, c]
        return rcopy(ref, ref, snd.at[7], wxr.at[k, 0], at(z, x + d, c))

    def wu_x2(k):
        ref = wu.at[hand_blk(k), lax.rem(x - toward + NX, NX), c]
        return rcopy(ref, ref, snd.at[8], wxr.at[k, 1], at(z, x + toward, c))

    def wg_x(i, xx):
        return rcopy(wg.at[z, xx, c], wg.at[z, xx, c], snd.at[9], one.at[1], at(z, x + DX[i], c))

    def got(ref, sem):
        rcopy(ref, ref, snd.at[0], sem, mate).wait_recv()

    def gone(ref, n):
        rcopy(ref, ref, snd.at[n], one.at[0], mate).wait_send()

    def from_x(i):
        return lax.rem(x - DX[i] + NX, NX)

    def ring_start(ring):
        ring[0](1).start()
        ring[1](1).start()

    def ring_step(ring, s, hand):
        def p():
            ring[2](s).wait_recv()
            only(plus_n, s + 1, lambda: ring[0](s + 1).start())
            if s < 4:
                hand(s)
            else:
                hand(7)

        def n():
            ring[3](s).wait_recv()
            only(minus_n, s + 1, lambda: ring[1](s + 1).start())
            if s < 4:
                hand(3 + s)
            else:
                hand(7)

        only(plus_n, s, p)
        only(minus_n, s, n)

    def ks(s):
        return (s, 3 + s) if s < 4 else (7,)

    def from_y(i):
        return lax.rem(y - DX[i] + NY, NY)

    half_cols = ow.shape[2] // 2

    def ow_y(i, yy):
        ref = ow.at[yy, :, pl.ds(pl.multiple_of(c * half_cols, 128), half_cols)]
        return rcopy(ref, ref, snd.at[10], one.at[2], across[i])

    def ow_hand(i, lane):
        ref = ow.at[from_y(i), :, pl.ds(pl.multiple_of(lane * half_cols, 128), half_cols)]
        return rcopy(ref, ref, snd.at[11], one.at[3], mate)

    def heads_y(i, yy):
        return rcopy(heads.at[yy], heads.at[yy], snd.at[12], hsr.at[i], across[i])

    def edge_copy():
        return rcopy(edge_out, edge_in, snd.at[13], one.at[5], after)

    def down_y(i, n):
        return rcopy(
            part.at[n, across[i][1]], drecv.at[i, n], snd.at[14], dyr.at[n], across[i]
        )

    for i in range(3):
        q_copy(i, x).start()
    ring_start(kv_rings[0])
    ring_start(kv_rings[1])
    kv_hand(0, c).start()
    for d in loads[5:9]:
        d.wait()
    for i in range(3):
        ow_y(i, y).start()
    ring_start(wu_ring)

    lane = lax.broadcasted_iota(jnp.int32, (ROWS, 128), 1)

    def prepare(slot):
        for half in range(2):
            block = q[slot, :, half * 128 : (half + 1) * 128] * bf16(0.125)
            zero = jnp.zeros_like(block)
            qz[half, slot, 0:ROWS] = jnp.where(lane < 64, block, zero)
            qz[half, slot, ROWS : 2 * ROWS] = jnp.where(lane < 64, zero, block)

    prepare(x)
    ring_step(kv_rings[0], 1, lambda k: None)
    for i in range(3):
        wg_x(i, x).start()
    wu_x(0, 1).start()
    wu_x(0, 3).start()
    ring_step(kv_rings[1], 1, lambda k: kv_hand(k, c).start())
    got(q.at[0:3], one.at[0])
    for i in range(3):
        prepare(from_x(i))

    def piece(chunk, pair, slot, masked):
        if masked:
            j = lax.broadcasted_iota(jnp.int32, (1, 768), 1)
            second = (j >= 384).astype(jnp.int32)
            core = ((j - 384 * second) >= 192).astype(jnp.int32)
            off = j - 384 * second - 192 * core
            key_pos = ((2 * pair + second) * 8 + x * 2 + core) * ROWS + off
            i = lax.broadcasted_iota(jnp.int32, (2 * ROWS, 1), 0)
            i = i - ROWS * (i >= ROWS).astype(jnp.int32)
            query_pos = (z * 8 + slot * 2 + c) * ROWS + i
            visible = key_pos <= query_pos
        for half in range(2):
            keys = kv[pl.ds(2 * pair, 2), :, :, half * 128 : (half + 1) * 128].reshape(768, 128)
            s = lax.dot_general(
                qz[half, slot], keys, (((1,), (1,)), ((), ())), preferred_element_type=f32
            )
            if masked:
                s = jnp.where(visible, s, HIDE)
            new = jnp.broadcast_to(
                jnp.maximum(jnp.max(s, axis=1, keepdims=True), FLOOR), (2 * ROWS, 128)
            )
            m[chunk, half, slot] = new
            e = jnp.exp(s - new[:, 0:1])
            part_sum = e[:, 0:128]
            for t in range(1, 6):
                part_sum = part_sum + e[:, t * 128 : (t + 1) * 128]
            l[chunk, half, slot] = part_sum
            eb = e.astype(bf16)
            for h in range(2):
                rows = slice(h * ROWS, (h + 1) * ROWS)
                vals = kv[pl.ds(2 * pair, 2), :, :, 256 + h * 128 : 384 + h * 128].reshape(768, 128)
                acc[chunk, half, slot, rows] = jnp.dot(eb[rows], vals, preferred_element_type=f32)

    def unseen(chunk, slot):
        for half in range(2):
            m[chunk, half, slot] = jnp.full((2 * ROWS, 128), FLOOR, f32)
            l[chunk, half, slot] = jnp.zeros((2 * ROWS, 128), f32)
            acc[chunk, half, slot] = jnp.zeros((2 * ROWS, 128), f32)

    own = z // 2
    odd = z % 2
    pairs = (
        own,
        lax.rem(own + jnp.where(odd == 1, 1, 3), 4),
        lax.rem(own + jnp.where(odd == 1, 3, 1), 4),
        lax.rem(own + 2, 4),
    )

    def join(slot, take_values):
        st = jnp.zeros((ROWS, 128), f32)
        for half in range(2):
            for h in range(2):
                rows = slice(h * ROWS, (h + 1) * ROWS)
                k = half * 2 + h
                ms = [m[n, half, slot, rows] for n in range(4)]
                top = jnp.maximum(jnp.maximum(ms[0], ms[1]), jnp.maximum(ms[2], ms[3]))
                tot, val = None, None
                for n in range(4):
                    w = jnp.exp(ms[n] - top)
                    t = l[n, half, slot, rows] * w
                    v = acc[n, half, slot, rows] * w
                    tot, val = (t, v) if n == 0 else (tot + t, val + v)
                take_values(half, h, val)
                st = jnp.where(lane == k, top, st)
                st = jnp.where(lane == 4 + k, jnp.sum(tot, axis=1, keepdims=True), st)
        return st

    def p_copy(i):
        return rcopy(psend.at[i], precv.at[i], snd.at[15], one.at[6], (at(z, x + i_dx(i), c)))

    def s_copy(i):
        return rcopy(ssend.at[i], srecv.at[i], snd.at[16], one.at[7], (at(z, x + i_dx(i), c)))

    def i_dx(i):
        return jnp.where(i == 0, 2, jnp.where(i == 1, 1, 3))

    def wu_spread(k):
        wu_x(k, 1).start()
        wu_x(k, 3).start()

    def wu_mid(k):
        got(wu.at[0, 0:2, c], wxr.at[k, 0])
        wu_x2(k).start()

    def wu_finish(k):
        got(wu.at[0, 0, c], wxr.at[k, 1])
        wu_hand(k, c).start()

    def kv_arrive(s, h):
        ring_step(kv_rings[h], s, lambda k: kv_hand(k, c).start() if h == 1 else None)

    def wu_arrive(s, spread):
        ring_step(wu_ring, s, lambda k: None)
        for k in spread:
            wu_spread(k)

    def all_slots(chunk, masked, first, s):
        pair = pairs[chunk]

        def body(slot, carry):
            if masked:
                piece(chunk, pair, slot, True)
            else:
                seen = pair < own
                pl.when(seen)(lambda: piece(chunk, pair, slot, False))
                pl.when(jnp.logical_not(seen))(lambda: unseen(chunk, slot))
            pl.when(slot == 0)(first)
            pl.when(slot == 1)(lambda: kv_arrive(s, 0))
            pl.when(slot == (3 if masked else 2))(lambda: kv_arrive(s, 1))
            return carry

        lax.fori_loop(0, NX, body, 0)

    for k in (0,) + ks(1):
        kv_hand(k, 1 - c).wait_recv()
    all_slots(0, True, lambda: wu_arrive(1, ks(1)), 2)
    got(wg.at[0, 0:3, c], one.at[1])
    wg_hand(0, c).start()
    wu_mid(0)
    for k in ks(2):
        kv_hand(k, 1 - c).wait_recv()
    all_slots(1, False, lambda: wu_arrive(2, ks(2)), 3)
    for k in ks(3):
        kv_hand(k, 1 - c).wait_recv()

    def last(idx, carry):
        final = jnp.logical_and(idx >= 3, idx != 6)
        i = jnp.where(idx < 3, idx, jnp.where(idx < 6, idx - 3, 3))
        slot = lax.rem(x + jnp.where(i == 3, 0, i_dx(i)), NX)
        chunk = jnp.where(final, 3, 2)
        pair = jnp.where(final, pairs[3], pairs[2])

        @pl.when(idx == 3)
        def _():
            for k in ks(4):
                kv_hand(k, 1 - c).wait_recv()

        seen = pair < own
        pl.when(seen)(lambda: piece(chunk, pair, slot, False))
        pl.when(jnp.logical_not(seen))(lambda: unseen(chunk, slot))

        @pl.when(jnp.logical_and(final, i < 3))
        def _():
            def put(half, h, val):
                col = (half * 2 + h) * 128
                psend[i, :, col : col + 128] = val.astype(bf16)

            st = jnp.concatenate((join(slot, put), jnp.zeros((64, 128), f32)), axis=0)
            ssend[i] = st.T[0:8]
            p_copy(i).start()
            s_copy(i).start()

        @pl.when(idx == 0)
        def _():
            wu_arrive(3, ())
            for ring in wg_rings:
                ring_start(ring)

        @pl.when(idx == 1)
        def _():
            wu_finish(0)
            for k in ks(1):
                wu_mid(k)

        @pl.when(idx == 2)
        def _():
            kv_arrive(4, 0)
            kv_arrive(4, 1)
            for k in ks(2):
                wu_mid(k)

        @pl.when(idx == 3)
        def _():
            wu_arrive(4, ())
            wg_step(0, 1)

        for j in (1, 2, 3):
            @pl.when(idx == 3 + j)
            def _():
                wg_step(j, 1)

        @pl.when(idx == 5)
        def _():
            for k in ks(1):
                wu_finish(k)

        @pl.when(idx == 6)
        def _():
            for k in ks(2):
                wu_finish(k)

        @pl.when(idx == 7)
        def _():
            wg_step(0, 2)

        return carry

    lax.fori_loop(0, 8, last, 0)
    for k in (3, 6, 7):
        wu_spread(k)
    wg_step(1, 2)
    wg_step(2, 2)
    wg_step(3, 2)
    got(ow.at[0:3, :, 0:half_cols], one.at[2])
    for i in range(3):
        ow_hand(i, c).start()

    def take(i):
        st = jnp.concatenate((srecv[i], jnp.zeros((120, 256), f32)), axis=0).T[0:ROWS]
        return st

    mine = {}

    def keep(half, h, val):
        mine[half, h] = val

    stats = [join(x, keep)]
    got(precv, one.at[6])
    got(srecv, one.at[7])
    stats += [take(i) for i in range(3)]
    for h in range(2):
        parts = []
        for half in range(2):
            k = half * 2 + h
            col = k * 128
            ms = [st[:, k : k + 1] for st in stats]
            ls = [st[:, 4 + k : 5 + k] for st in stats]
            top = functools.reduce(jnp.maximum, ms)
            ws = [jnp.exp(a - top) for a in ms]
            tot = sum(w * t for w, t in zip(ws, ls))
            joined = mine[half, h] * ws[0]
            for i in range(3):
                joined = joined + precv[i, :, col : col + 128].astype(f32) * ws[i + 1]
            parts.append(joined / tot)
        diff = parts[0] - lam[h] * parts[1]
        heads[y, :, h * 128 : (h + 1) * 128] = rms_scale(diff, gain[...]).astype(bf16)

    for i in range(3):
        heads_y(i, y).start()

    wg_step(0, 3)
    wu_mid(3)
    wg_step(1, 3)
    wg_step(2, 3)
    wg_step(3, 3)
    wu_mid(6)

    loads[9].wait()
    loads[10].wait()
    got(ow.at[0:3, :, 0:half_cols], one.at[3])
    width = stream.shape[2]
    for i in (None, 1, 2, 0):
        yy = y
        if i is not None:
            yy = from_y(i)
            heads_y(i, yy).wait_recv()
        for n in range(0, width, 512):
            cols = slice(n, n + 512)
            more = jnp.dot(heads[yy], ow[yy, :, cols], preferred_element_type=f32)
            more = more.reshape(NY, ROWS // NY, 512)
            if i is None:
                more = more + res[:, cols].astype(f32).reshape(NY, ROWS // NY, 512)
            else:
                more = more + stream[:, :, cols]
            stream[:, :, cols] = more
    rows = stream[...].reshape(ROWS, width)
    normed = rms_scale(rows, mix_gain[...]).astype(bf16)
    for zz in range(NZ):
        ffn[zz] = normed[:, zz * 256 : (zz + 1) * 256]

    order = (0,) + ks(1) + ks(2) + ks(3) + ks(4)
    pieces = ((wg, slice(0, cut)), (wu, slice(cut, 2 * ff)))
    for n in range(0, 8, 2):
        two = order[n : n + 2]
        if n == 0:
            wg_step(0, 4)
            wu_mid(7)
        if n == 2:
            wg_step(1, 4)
            wg_step(2, 4)
            wu_finish(3)
        if n == 4:
            wu_finish(6)
            wg_step(3, 4)
            wu_finish(7)
        for k in two:
            wg_hand(k, 1 - c).wait_recv()
            wu_hand(k, 1 - c).wait_recv()
        blks = [hand_blk(k) for k in two]

        def product(w, top):
            return sum(
                jnp.dot(ffn[b, top:], w[b].reshape(256, -1), preferred_element_type=f32)
                for b in blks
            )

        if n == 6:
            for w, cols in pieces:
                tip = product(w, ROWS - 16)
                tip = (tip[8:] + pad[ROWS : 8 + ROWS, cols]).astype(bf16).astype(f32)
                edge_out[:, cols] = tip[6:8]
            edge_copy().start()
        for w, cols in pieces:
            pre = product(w, 0)
            if n > 0:
                pre = pre + pad[8 : 8 + ROWS, cols]
            if n == 6:
                pre = pre.astype(bf16).astype(f32)
            pad[8 : 8 + ROWS, cols] = pre

    def mix(top, size):
        for n in range(0, ff, 128):
            cols = slice(n, n + 128)
            conv = []
            for base, taps in ((0, gate_taps), (ff, up_taps)):
                there = slice(base + n, base + n + 128)
                v = taps[0:1, cols] * pad[6 + top : 6 + top + size, there]
                v = v + taps[1:2, cols] * pad[7 + top : 7 + top + size, there]
                v = v + taps[2:3, cols] * pad[8 + top : 8 + top + size, there]
                conv.append(v)
            hidden[top : top + size, cols] = (jax.nn.silu(conv[0]) * conv[1]).astype(bf16)

    mix(16, ROWS - 16)
    edge_copy().wait_recv()
    pad[6:8, :] = jnp.where(r == 0, 0.0, edge_in[...])
    mix(0, 16)

    for n in range(NY):
        cols = slice(n * 512, (n + 1) * 512)
        down = jnp.dot(hidden[...], dw[:, cols], preferred_element_type=f32)
        part[n] = down.astype(bf16).reshape(NY, ROWS // NY, 512)
        for i in range(3):
            down_y(i, n).start()
    edge_copy().wait_send()
    gone(q.at[0:3], 0)
    gone(kv.at[0:7, 0], 1)
    gone(wu.at[0:7, 0, 0], 2)
    gone(wg.at[0:7, :, 0], 3)
    gone(kv.at[:, 0], 4)
    gone(wg.at[:, :, 0], 5)
    gone(wu.at[:, :, 0], 6)
    gone(wu.at[:, 0:2, 0], 7)
    gone(wu.at[:, 0, 0], 8)
    gone(wg.at[0, 0:3, 0], 9)
    gone(ow.at[0:3, :, 0:half_cols], 10)
    gone(ow.at[0:3, :, 0:half_cols], 11)
    gone(heads.at[0:3], 12)
    gone(psend, 15)
    gone(ssend, 16)
    for n in range(NY):
        cols = slice(n * 512, (n + 1) * 512)
        total = stream[y, :, cols] + part[n, y].astype(f32)
        got(drecv.at[:, n], dyr.at[n])
        for i in range(3):
            total = total + drecv[i, n].astype(f32)
        out[:, cols] = total.astype(bf16)
    gone(drecv, 14)


def layer(*args):
    ANY = pl.BlockSpec(memory_space=pl.ANY)
    VM = pl.BlockSpec(memory_space=pltpu.VMEM)
    SM = pl.BlockSpec(memory_space=pltpu.SMEM)
    ff, width = args[5].shape[1], args[8].shape[1]
    dma = pltpu.SemaphoreType.DMA
    cut = 9 * 128 if ff > 9 * 128 else ff // 2
    sems = [(11,), (17,), (8,), (3,), (2, 2, 4), (8,), (2, 4), (8, 2), (8,), (NX, 2, 4), (8,), (NY,)]
    return pl.pallas_call(
        layer_kernel,
        out_shape=jax.ShapeDtypeStruct((ROWS // NY, width), bf16),
        in_specs=[ANY] * 10 + [SM] + [VM] * 4,
        out_specs=VM,
        scratch_shapes=[
            pltpu.VMEM((4, ROWS, 256), bf16),
            pltpu.VMEM((8, 2, ROWS, 512), bf16),
            pltpu.VMEM((8, 4, 2, 32, cut), bf16),
            pltpu.VMEM((8, 4, 2, 32, 2 * ff - cut), bf16),
            pltpu.VMEM((2, 4, 2 * ROWS, 128), bf16),
            pltpu.VMEM((4, 2, 4, 2 * ROWS, 128), f32),
            pltpu.VMEM((4, 2, 4, 2 * ROWS, 128), f32),
            pltpu.VMEM((4, 2, 4, 2 * ROWS, 128), f32),
            pltpu.VMEM((3, ROWS, 512), bf16),
            pltpu.VMEM((3, ROWS, 512), bf16),
            pltpu.VMEM((3, 8, 256), f32),
            pltpu.VMEM((3, 8, 256), f32),
            pltpu.VMEM((NY, ROWS, 256), bf16),
            pltpu.VMEM((NY, 256, width), bf16),
            pltpu.VMEM((ff, width), bf16),
            pltpu.VMEM((ROWS, width), bf16),
            pltpu.VMEM((NY, ROWS // NY, width), f32),
            pltpu.VMEM((NZ, ROWS, 256), bf16),
            pltpu.VMEM((8 + ROWS, 2 * ff), f32),
            pltpu.VMEM((ROWS, ff), bf16),
            pltpu.VMEM((2, 2 * ff), f32),
            pltpu.VMEM((2, 2 * ff), f32),
            pltpu.VMEM((NY, NY, ROWS // NY, 512), bf16),
            pltpu.VMEM((3, NY, ROWS // NY, 512), bf16),
        ] + [dma(s) for s in sems],
        compiler_params=pltpu.CompilerParams(
            collective_id=0, has_side_effects=True, vmem_limit_bytes=63 * 1024 * 1024
        ),
        name="layer",
    )(*args)


def shards(
    q_first, k_first, q_second, k_second, values, lambdas, head_gain, out_weight, residual_in,
    mix_gain, gate_weight, up_weight, gate_taps, up_taps, down_weight,
):
    return layer(
        q_first, q_second, k_first, k_second, values, gate_weight, up_weight, out_weight,
        residual_in, down_weight, lambdas, head_gain[None], mix_gain[None], gate_taps, up_taps,
    )


def solution(mesh):
    in_specs = (
        P("sp", "tp"), P("sp", "tp"), P("sp", "tp"), P("sp", "tp"), P("sp", "tp"),
        P("tp"), P(), P("tp", None), P("sp", None), P(),
        P("sp", "tp"), P("sp", "tp"), P(None, "tp"), P(None, "tp"), P("tp", None),
    )
    out_specs = P(("sp", "tp"), None)
    return jax.shard_map(shards, mesh=mesh, in_specs=in_specs, out_specs=out_specs, check_vma=False)
```

```python
import functools

import jax
import jax.numpy as jnp
from jax import lax
from jax.experimental import pallas as pl
from jax.experimental.pallas import tpu as pltpu
from jax.sharding import PartitionSpec as P

MESH = pl.DeviceIdType.MESH
norm_eps = 1e-06
ROWS = 192
NX, NZ, NY = 4, 8, 4
DX = (2, 1, 3)
HIDE = -2e30
FLOOR = -1e30
f32, bf16 = jnp.float32, jnp.bfloat16


def rms_scale(field, gain):
    return field * lax.rsqrt(jnp.mean(field * field, axis=-1, keepdims=True) + norm_eps) * gain


def layer_kernel(
    qa, qb, ka, kb, va, gw, uw, out_w, res_in, down_w, lam, gain, mix_gain, gate_taps, up_taps,
    out,
    q, kv, wg, wu, qz, m, l, acc, psend, precv, ssend, srecv,
    heads, ow, dw, res, stream, ffn, pad, hidden, edge_out, edge_in, part, drecv,
    loc, snd, one, hsr, kvr, kdr, wur, wxr, wdr, gzr, gdr, dyr,
):
    r = lax.axis_index("sp")
    y = lax.axis_index("tp")
    z, x, c = r // 8, (r // 2) % 4, r % 2

    def at(zz, xx, cc):
        return (lax.rem(zz + NZ, NZ) * 8 + lax.rem(xx + NX, NX) * 2 + cc, y)

    mate = (r + 1 - 2 * c, y)
    up_dev, down_dev = at(z + 1, x, c), at(z - 1, x, c)

    def rcopy(src, dst, ss, rs, dev):
        return pltpu.make_async_remote_copy(
            src_ref=src, dst_ref=dst, send_sem=ss, recv_sem=rs, device_id=dev, device_id_type=MESH
        )

    cut, ff = wg.shape[4], hidden.shape[1]
    loads = [
        (qa, q.at[x, :, 0:128]),
        (qb, q.at[x, :, 128:256]),
        (ka, kv.at[z, c, :, 0:128]),
        (kb, kv.at[z, c, :, 128:256]),
        (va, kv.at[z, c, :, 256:512]),
        (gw.at[:, 0:cut], wg.at[z, x, c]),
        (gw.at[:, cut:ff], wu.at[z, x, c, :, 0 : ff - cut]),
        (uw, wu.at[z, x, c, :, ff - cut : 2 * ff - cut]),
        (out_w, ow.at[y]),
        (res_in, res),
        (down_w, dw),
    ]
    loads = [pltpu.make_async_copy(s, d, loc.at[i]) for i, (s, d) in enumerate(loads)]
    for d in loads:
        d.start()
    barrier = pltpu.get_barrier_semaphore()
    across = [(r, lax.rem(y + d, NY)) for d in DX]
    after, before = (lax.rem(r + 1, 64), y), (lax.rem(r + 63, 64), y)
    greeted = [up_dev, down_dev, mate, after, before] + [at(z, x + d, c) for d in DX] + across
    for dev in greeted:
        pl.semaphore_signal(barrier, inc=1, device_id=dev, device_id_type=MESH)
    pl.semaphore_wait(barrier, len(greeted))
    for d in loads[:5]:
        d.wait()

    def q_copy(i, slot):
        return rcopy(q.at[slot], q.at[slot], snd.at[0], one.at[0], at(z, x + DX[i], c))

    plus_n, minus_n = 4 - c, 3 + c

    def z_ring(ref_at, sends, recvs):
        def plus(s):
            blk = lax.rem(z - s + 1 + NZ, NZ)
            return rcopy(ref_at(blk), ref_at(blk), sends, recvs.at[0, s - 1], up_dev)

        def minus(s):
            blk = lax.rem(z + s - 1, NZ)
            return rcopy(ref_at(blk), ref_at(blk), sends, recvs.at[1, s - 1], down_dev)

        def plus_in(s):
            blk = lax.rem(z - s + NZ, NZ)
            return rcopy(ref_at(blk), ref_at(blk), sends, recvs.at[0, s - 1], up_dev)

        def minus_in(s):
            blk = lax.rem(z + s, NZ)
            return rcopy(ref_at(blk), ref_at(blk), sends, recvs.at[1, s - 1], down_dev)

        return plus, minus, plus_in, minus_in

    def only(n, s, fn):
        if s <= 3:
            fn()
        elif s == 4:
            pl.when(n == 4)(fn)

    kv_rings = [
        z_ring(lambda b, h=h: kv.at[b, c, h * 96 : (h + 1) * 96], snd.at[1], kvr.at[h])
        for h in range(2)
    ]
    wu_ring = z_ring(lambda b: wu.at[b, x, c], snd.at[2], wur)
    wg_rings = [
        z_ring(lambda b, j=j: wg.at[b, lax.rem(x + j, NX), c], snd.at[3], gzr.at[j])
        for j in range(NX)
    ]

    def wg_step(j, s):
        ring_step(wg_rings[j], s, lambda k: None)
        if j == NX - 1:
            for k in ks(s):
                wg_hand(k, c).start()


    def hand_blk(k):
        off = (0, -1, -2, -3, 1, 2, 3, 4)[k]
        return lax.rem(z + off + NZ, NZ)

    def kv_hand(k, lane):
        b = hand_blk(k)
        return rcopy(kv.at[b, lane], kv.at[b, lane], snd.at[4], kdr.at[k], mate)

    def wg_hand(k, lane):
        b = hand_blk(k)
        return rcopy(wg.at[b, :, lane], wg.at[b, :, lane], snd.at[5], gdr.at[k], mate)

    def wu_hand(k, lane):
        b = hand_blk(k)
        return rcopy(wu.at[b, :, lane], wu.at[b, :, lane], snd.at[6], wdr.at[k], mate)

    toward = 1 - 2 * c

    def wu_x(k, d):
        ref = wu.at[hand_blk(k), x, c]
        return rcopy(ref, ref, snd.at[7], wxr.at[k, 0], at(z, x + d, c))

    def wu_x2(k):
        ref = wu.at[hand_blk(k), lax.rem(x - toward + NX, NX), c]
        return rcopy(ref, ref, snd.at[8], wxr.at[k, 1], at(z, x + toward, c))

    def wg_x(i, xx):
        return rcopy(wg.at[z, xx, c], wg.at[z, xx, c], snd.at[9], one.at[1], at(z, x + DX[i], c))

    def got(ref, sem):
        rcopy(ref, ref, snd.at[0], sem, mate).wait_recv()

    def gone(ref, n):
        rcopy(ref, ref, snd.at[n], one.at[0], mate).wait_send()

    def from_x(i):
        return lax.rem(x - DX[i] + NX, NX)

    def ring_start(ring):
        ring[0](1).start()
        ring[1](1).start()

    def ring_step(ring, s, hand):
        def p():
            ring[2](s).wait_recv()
            only(plus_n, s + 1, lambda: ring[0](s + 1).start())
            if s < 4:
                hand(s)
            else:
                hand(7)

        def n():
            ring[3](s).wait_recv()
            only(minus_n, s + 1, lambda: ring[1](s + 1).start())
            if s < 4:
                hand(3 + s)
            else:
                hand(7)

        only(plus_n, s, p)
        only(minus_n, s, n)

    def ks(s):
        return (s, 3 + s) if s < 4 else (7,)

    def from_y(i):
        return lax.rem(y - DX[i] + NY, NY)

    half_cols = ow.shape[2] // 2

    def ow_y(i, yy):
        ref = ow.at[yy, :, pl.ds(pl.multiple_of(c * half_cols, 128), half_cols)]
        return rcopy(ref, ref, snd.at[10], one.at[2], across[i])

    def ow_hand(i, lane):
        ref = ow.at[from_y(i), :, pl.ds(pl.multiple_of(lane * half_cols, 128), half_cols)]
        return rcopy(ref, ref, snd.at[11], one.at[3], mate)

    def heads_y(i, yy):
        return rcopy(heads.at[yy], heads.at[yy], snd.at[12], hsr.at[i], across[i])

    def edge_copy():
        return rcopy(edge_out, edge_in, snd.at[13], one.at[5], after)

    def down_y(i, n):
        return rcopy(
            part.at[n, across[i][1]], drecv.at[i, n], snd.at[14], dyr.at[n], across[i]
        )

    for i in range(3):
        q_copy(i, x).start()
    ring_start(kv_rings[0])
    ring_start(kv_rings[1])
    kv_hand(0, c).start()
    for d in loads[5:9]:
        d.wait()
    for i in range(3):
        ow_y(i, y).start()
    ring_start(wu_ring)

    lane = lax.broadcasted_iota(jnp.int32, (ROWS, 128), 1)

    def prepare(slot):
        for half in range(2):
            block = q[slot, :, half * 128 : (half + 1) * 128] * bf16(0.125)
            zero = jnp.zeros_like(block)
            qz[half, slot, 0:ROWS] = jnp.where(lane < 64, block, zero)
            qz[half, slot, ROWS : 2 * ROWS] = jnp.where(lane < 64, zero, block)

    prepare(x)
    ring_step(kv_rings[0], 1, lambda k: None)
    for i in range(3):
        wg_x(i, x).start()
    wu_x(0, 1).start()
    wu_x(0, 3).start()
    ring_step(kv_rings[1], 1, lambda k: kv_hand(k, c).start())
    got(q.at[0:3], one.at[0])
    for i in range(3):
        prepare(from_x(i))

    def piece(chunk, pair, slot, masked):
        if masked:
            j = lax.broadcasted_iota(jnp.int32, (1, 768), 1)
            second = (j >= 384).astype(jnp.int32)
            core = ((j - 384 * second) >= 192).astype(jnp.int32)
            off = j - 384 * second - 192 * core
            key_pos = ((2 * pair + second) * 8 + x * 2 + core) * ROWS + off
            i = lax.broadcasted_iota(jnp.int32, (2 * ROWS, 1), 0)
            i = i - ROWS * (i >= ROWS).astype(jnp.int32)
            query_pos = (z * 8 + slot * 2 + c) * ROWS + i
            visible = key_pos <= query_pos
        for half in range(2):
            keys = kv[pl.ds(2 * pair, 2), :, :, half * 128 : (half + 1) * 128].reshape(768, 128)
            s = lax.dot_general(
                qz[half, slot], keys, (((1,), (1,)), ((), ())), preferred_element_type=f32
            )
            if masked:
                s = jnp.where(visible, s, HIDE)
            new = jnp.broadcast_to(
                jnp.maximum(jnp.max(s, axis=1, keepdims=True), FLOOR), (2 * ROWS, 128)
            )
            m[chunk, half, slot] = new
            e = jnp.exp(s - new[:, 0:1])
            part_sum = e[:, 0:128]
            for t in range(1, 6):
                part_sum = part_sum + e[:, t * 128 : (t + 1) * 128]
            l[chunk, half, slot] = part_sum
            eb = e.astype(bf16)
            for h in range(2):
                rows = slice(h * ROWS, (h + 1) * ROWS)
                vals = kv[pl.ds(2 * pair, 2), :, :, 256 + h * 128 : 384 + h * 128].reshape(768, 128)
                acc[chunk, half, slot, rows] = jnp.dot(eb[rows], vals, preferred_element_type=f32)

    def unseen(chunk, slot):
        for half in range(2):
            m[chunk, half, slot] = jnp.full((2 * ROWS, 128), FLOOR, f32)
            l[chunk, half, slot] = jnp.zeros((2 * ROWS, 128), f32)
            acc[chunk, half, slot] = jnp.zeros((2 * ROWS, 128), f32)

    own = z // 2
    odd = z % 2
    pairs = (
        own,
        lax.rem(own + jnp.where(odd == 1, 1, 3), 4),
        lax.rem(own + jnp.where(odd == 1, 3, 1), 4),
        lax.rem(own + 2, 4),
    )

    def join(slot, take_values):
        st = jnp.zeros((ROWS, 128), f32)
        for half in range(2):
            for h in range(2):
                rows = slice(h * ROWS, (h + 1) * ROWS)
                k = half * 2 + h
                ms = [m[n, half, slot, rows] for n in range(4)]
                top = jnp.maximum(jnp.maximum(ms[0], ms[1]), jnp.maximum(ms[2], ms[3]))
                tot, val = None, None
                for n in range(4):
                    w = jnp.exp(ms[n] - top)
                    t = l[n, half, slot, rows] * w
                    v = acc[n, half, slot, rows] * w
                    tot, val = (t, v) if n == 0 else (tot + t, val + v)
                take_values(half, h, val)
                st = jnp.where(lane == k, top, st)
                st = jnp.where(lane == 4 + k, jnp.sum(tot, axis=1, keepdims=True), st)
        return st

    def p_copy(i):
        return rcopy(psend.at[i], precv.at[i], snd.at[15], one.at[6], (at(z, x + i_dx(i), c)))

    def s_copy(i):
        return rcopy(ssend.at[i], srecv.at[i], snd.at[16], one.at[7], (at(z, x + i_dx(i), c)))

    def i_dx(i):
        return jnp.where(i == 0, 2, jnp.where(i == 1, 1, 3))

    def wu_spread(k):
        wu_x(k, 1).start()
        wu_x(k, 3).start()

    def wu_mid(k):
        got(wu.at[0, 0:2, c], wxr.at[k, 0])
        wu_x2(k).start()

    def wu_finish(k):
        got(wu.at[0, 0, c], wxr.at[k, 1])
        wu_hand(k, c).start()

    def kv_arrive(s, h):
        ring_step(kv_rings[h], s, lambda k: kv_hand(k, c).start() if h == 1 else None)

    def wu_arrive(s, spread):
        ring_step(wu_ring, s, lambda k: None)
        for k in spread:
            wu_spread(k)

    def all_slots(chunk, masked, first, s):
        pair = pairs[chunk]

        def body(slot, carry):
            if masked:
                piece(chunk, pair, slot, True)
            else:
                seen = pair < own
                pl.when(seen)(lambda: piece(chunk, pair, slot, False))
                pl.when(jnp.logical_not(seen))(lambda: unseen(chunk, slot))
            pl.when(slot == 0)(first)
            pl.when(slot == 1)(lambda: kv_arrive(s, 0))
            pl.when(slot == (3 if masked else 2))(lambda: kv_arrive(s, 1))
            return carry

        lax.fori_loop(0, NX, body, 0)

    for k in (0,) + ks(1):
        kv_hand(k, 1 - c).wait_recv()
    all_slots(0, True, lambda: wu_arrive(1, ks(1)), 2)
    got(wg.at[0, 0:3, c], one.at[1])
    wg_hand(0, c).start()
    wu_mid(0)
    for k in ks(2):
        kv_hand(k, 1 - c).wait_recv()
    all_slots(1, False, lambda: wu_arrive(2, ks(2)), 3)
    for k in ks(3):
        kv_hand(k, 1 - c).wait_recv()

    def last(idx, carry):
        final = jnp.logical_and(idx >= 3, idx != 6)
        i = jnp.where(idx < 3, idx, jnp.where(idx < 6, idx - 3, 3))
        slot = lax.rem(x + jnp.where(i == 3, 0, i_dx(i)), NX)
        chunk = jnp.where(final, 3, 2)
        pair = jnp.where(final, pairs[3], pairs[2])

        @pl.when(idx == 3)
        def _():
            for k in ks(4):
                kv_hand(k, 1 - c).wait_recv()

        seen = pair < own
        pl.when(seen)(lambda: piece(chunk, pair, slot, False))
        pl.when(jnp.logical_not(seen))(lambda: unseen(chunk, slot))

        @pl.when(jnp.logical_and(final, i < 3))
        def _():
            def put(half, h, val):
                col = (half * 2 + h) * 128
                psend[i, :, col : col + 128] = val.astype(bf16)

            st = jnp.concatenate((join(slot, put), jnp.zeros((64, 128), f32)), axis=0)
            ssend[i] = st.T[0:8]
            p_copy(i).start()
            s_copy(i).start()

        @pl.when(idx == 0)
        def _():
            wu_arrive(3, ())
            for ring in wg_rings:
                ring_start(ring)

        @pl.when(idx == 1)
        def _():
            wu_finish(0)
            for k in ks(1):
                wu_mid(k)

        @pl.when(idx == 2)
        def _():
            kv_arrive(4, 0)
            kv_arrive(4, 1)
            for k in ks(2):
                wu_mid(k)

        @pl.when(idx == 3)
        def _():
            wu_arrive(4, ())
            wg_step(0, 1)

        for j in (1, 2, 3):
            @pl.when(idx == 3 + j)
            def _():
                wg_step(j, 1)

        @pl.when(idx == 5)
        def _():
            for k in ks(1):
                wu_finish(k)

        @pl.when(idx == 6)
        def _():
            for k in ks(2):
                wu_finish(k)

        @pl.when(idx == 7)
        def _():
            wg_step(0, 2)

        return carry

    lax.fori_loop(0, 8, last, 0)
    for k in (3, 6, 7):
        wu_spread(k)
    wg_step(1, 2)
    wg_step(2, 2)
    wg_step(3, 2)
    got(ow.at[0:3, :, 0:half_cols], one.at[2])
    for i in range(3):
        ow_hand(i, c).start()

    def take(i):
        st = jnp.concatenate((srecv[i], jnp.zeros((120, 256), f32)), axis=0).T[0:ROWS]
        return st

    mine = {}

    def keep(half, h, val):
        mine[half, h] = val

    stats = [join(x, keep)]
    got(precv, one.at[6])
    got(srecv, one.at[7])
    stats += [take(i) for i in range(3)]
    for h in range(2):
        parts = []
        for half in range(2):
            k = half * 2 + h
            col = k * 128
            ms = [st[:, k : k + 1] for st in stats]
            ls = [st[:, 4 + k : 5 + k] for st in stats]
            top = functools.reduce(jnp.maximum, ms)
            ws = [jnp.exp(a - top) for a in ms]
            tot = sum(w * t for w, t in zip(ws, ls))
            joined = mine[half, h] * ws[0]
            for i in range(3):
                joined = joined + precv[i, :, col : col + 128].astype(f32) * ws[i + 1]
            parts.append(joined / tot)
        diff = parts[0] - lam[h] * parts[1]
        heads[y, :, h * 128 : (h + 1) * 128] = rms_scale(diff, gain[...]).astype(bf16)

    for i in range(3):
        heads_y(i, y).start()

    wg_step(0, 3)
    wu_mid(3)
    wg_step(1, 3)
    wg_step(2, 3)
    wg_step(3, 3)
    wu_mid(6)

    loads[9].wait()
    loads[10].wait()
    got(ow.at[0:3, :, 0:half_cols], one.at[3])
    width = stream.shape[2]
    for i in (None, 1, 2, 0):
        yy = y
        if i is not None:
            yy = from_y(i)
            heads_y(i, yy).wait_recv()
        for n in range(0, width, 512):
            cols = slice(n, n + 512)
            more = jnp.dot(heads[yy], ow[yy, :, cols], preferred_element_type=f32)
            more = more.reshape(NY, ROWS // NY, 512)
            if i is None:
                more = more + res[:, cols].astype(f32).reshape(NY, ROWS // NY, 512)
            else:
                more = more + stream[:, :, cols]
            stream[:, :, cols] = more
    rows = stream[...].reshape(ROWS, width)
    normed = rms_scale(rows, mix_gain[...]).astype(bf16)
    for zz in range(NZ):
        ffn[zz] = normed[:, zz * 256 : (zz + 1) * 256]

    order = (0,) + ks(1) + ks(2) + ks(3) + ks(4)
    pieces = ((wg, slice(0, cut)), (wu, slice(cut, 2 * ff)))
    for n in range(0, 8, 2):
        two = order[n : n + 2]
        if n == 0:
            wg_step(0, 4)
            wu_mid(7)
        if n == 2:
            wg_step(1, 4)
            wg_step(2, 4)
            wu_finish(3)
        if n == 4:
            wu_finish(6)
            wg_step(3, 4)
            wu_finish(7)
        for k in two:
            wg_hand(k, 1 - c).wait_recv()
            wu_hand(k, 1 - c).wait_recv()
        blks = [hand_blk(k) for k in two]

        def product(w, top):
            return sum(
                jnp.dot(ffn[b, top:], w[b].reshape(256, -1), preferred_element_type=f32)
                for b in blks
            )

        if n == 6:
            for w, cols in pieces:
                tip = product(w, ROWS - 16)
                tip = (tip[8:] + pad[ROWS : 8 + ROWS, cols]).astype(bf16).astype(f32)
                edge_out[:, cols] = tip[6:8]
            edge_copy().start()
        for w, cols in pieces:
            pre = product(w, 0)
            if n > 0:
                pre = pre + pad[8 : 8 + ROWS, cols]
            if n == 6:
                pre = pre.astype(bf16).astype(f32)
            pad[8 : 8 + ROWS, cols] = pre

    def mix(top, size):
        for n in range(0, ff, 128):
            cols = slice(n, n + 128)
            conv = []
            for base, taps in ((0, gate_taps), (ff, up_taps)):
                there = slice(base + n, base + n + 128)
                v = taps[0:1, cols] * pad[6 + top : 6 + top + size, there]
                v = v + taps[1:2, cols] * pad[7 + top : 7 + top + size, there]
                v = v + taps[2:3, cols] * pad[8 + top : 8 + top + size, there]
                conv.append(v)
            hidden[top : top + size, cols] = (jax.nn.silu(conv[0]) * conv[1]).astype(bf16)

    mix(16, ROWS - 16)
    edge_copy().wait_recv()
    pad[6:8, :] = jnp.where(r == 0, 0.0, edge_in[...])
    mix(0, 16)

    for n in range(NY):
        cols = slice(n * 512, (n + 1) * 512)
        down = jnp.dot(hidden[...], dw[:, cols], preferred_element_type=f32)
        part[n] = down.astype(bf16).reshape(NY, ROWS // NY, 512)
        for i in range(3):
            down_y(i, n).start()
    edge_copy().wait_send()
    gone(q.at[0:3], 0)
    gone(kv.at[0:7, 0], 1)
    gone(wu.at[0:7, 0, 0], 2)
    gone(wg.at[0:7, :, 0], 3)
    gone(kv.at[:, 0], 4)
    gone(wg.at[:, :, 0], 5)
    gone(wu.at[:, :, 0], 6)
    gone(wu.at[:, 0:2, 0], 7)
    gone(wu.at[:, 0, 0], 8)
    gone(wg.at[0, 0:3, 0], 9)
    gone(ow.at[0:3, :, 0:half_cols], 10)
    gone(ow.at[0:3, :, 0:half_cols], 11)
    gone(heads.at[0:3], 12)
    gone(psend, 15)
    gone(ssend, 16)
    for n in range(NY):
        cols = slice(n * 512, (n + 1) * 512)
        total = stream[y, :, cols] + part[n, y].astype(f32)
        got(drecv.at[:, n], dyr.at[n])
        for i in range(3):
            total = total + drecv[i, n].astype(f32)
        out[:, cols] = total.astype(bf16)
    gone(drecv, 14)


def layer(*args):
    ANY = pl.BlockSpec(memory_space=pl.ANY)
    VM = pl.BlockSpec(memory_space=pltpu.VMEM)
    SM = pl.BlockSpec(memory_space=pltpu.SMEM)
    ff, width = args[5].shape[1], args[8].shape[1]
    dma = pltpu.SemaphoreType.DMA
    cut = 8 * 128 if ff > 8 * 128 else ff // 2
    sems = [(11,), (17,), (8,), (3,), (2, 2, 4), (8,), (2, 4), (8, 2), (8,), (NX, 2, 4), (8,), (NY,)]
    return pl.pallas_call(
        layer_kernel,
        out_shape=jax.ShapeDtypeStruct((ROWS // NY, width), bf16),
        in_specs=[ANY] * 10 + [SM] + [VM] * 4,
        out_specs=VM,
        scratch_shapes=[
            pltpu.VMEM((4, ROWS, 256), bf16),
            pltpu.VMEM((8, 2, ROWS, 512), bf16),
            pltpu.VMEM((8, 4, 2, 32, cut), bf16),
            pltpu.VMEM((8, 4, 2, 32, 2 * ff - cut), bf16),
            pltpu.VMEM((2, 4, 2 * ROWS, 128), bf16),
            pltpu.VMEM((4, 2, 4, 2 * ROWS, 128), f32),
            pltpu.VMEM((4, 2, 4, 2 * ROWS, 128), f32),
            pltpu.VMEM((4, 2, 4, 2 * ROWS, 128), f32),
            pltpu.VMEM((3, ROWS, 512), bf16),
            pltpu.VMEM((3, ROWS, 512), bf16),
            pltpu.VMEM((3, 8, 256), f32),
            pltpu.VMEM((3, 8, 256), f32),
            pltpu.VMEM((NY, ROWS, 256), bf16),
            pltpu.VMEM((NY, 256, width), bf16),
            pltpu.VMEM((ff, width), bf16),
            pltpu.VMEM((ROWS, width), bf16),
            pltpu.VMEM((NY, ROWS // NY, width), f32),
            pltpu.VMEM((NZ, ROWS, 256), bf16),
            pltpu.VMEM((8 + ROWS, 2 * ff), f32),
            pltpu.VMEM((ROWS, ff), bf16),
            pltpu.VMEM((2, 2 * ff), f32),
            pltpu.VMEM((2, 2 * ff), f32),
            pltpu.VMEM((NY, NY, ROWS // NY, 512), bf16),
            pltpu.VMEM((3, NY, ROWS // NY, 512), bf16),
        ] + [dma(s) for s in sems],
        compiler_params=pltpu.CompilerParams(
            collective_id=0, has_side_effects=True, vmem_limit_bytes=63 * 1024 * 1024
        ),
        name="layer",
    )(*args)


def shards(
    q_first, k_first, q_second, k_second, values, lambdas, head_gain, out_weight, residual_in,
    mix_gain, gate_weight, up_weight, gate_taps, up_taps, down_weight,
):
    return layer(
        q_first, q_second, k_first, k_second, values, gate_weight, up_weight, out_weight,
        residual_in, down_weight, lambdas, head_gain[None], mix_gain[None], gate_taps, up_taps,
    )


def solution(mesh):
    in_specs = (
        P("sp", "tp"), P("sp", "tp"), P("sp", "tp"), P("sp", "tp"), P("sp", "tp"),
        P("tp"), P(), P("tp", None), P("sp", None), P(),
        P("sp", "tp"), P("sp", "tp"), P(None, "tp"), P(None, "tp"), P("tp", None),
    )
    out_specs = P(("sp", "tp"), None)
    return jax.shard_map(shards, mesh=mesh, in_specs=in_specs, out_specs=out_specs, check_vma=False)
```

```python
import functools

import jax
import jax.numpy as jnp
from jax import lax
from jax.experimental import pallas as pl
from jax.experimental.pallas import tpu as pltpu
from jax.sharding import PartitionSpec as P

MESH = pl.DeviceIdType.MESH
norm_eps = 1e-06
ROWS = 192
NX, NZ, NY = 4, 8, 4
DX = (2, 1, 3)
HIDE = -2e30
FLOOR = -1e30
f32, bf16 = jnp.float32, jnp.bfloat16


def rms_scale(field, gain):
    return field * lax.rsqrt(jnp.mean(field * field, axis=-1, keepdims=True) + norm_eps) * gain


def layer_kernel(
    qa, qb, ka, kb, va, gw, uw, out_w, res_in, down_w, lam, gain, mix_gain, gate_taps, up_taps,
    out,
    q, kv, wg, wu, qz, m, l, acc, psend, precv, ssend, srecv,
    heads, ow, dw, res, stream, ffn, pad, hidden, edge_out, edge_in, part, drecv,
    loc, snd, one, hsr, kvr, kdr, wur, wxr, wdr, gzr, gdr, dyr,
):
    r = lax.axis_index("sp")
    y = lax.axis_index("tp")
    z, x, c = r // 8, (r // 2) % 4, r % 2

    def at(zz, xx, cc):
        return (lax.rem(zz + NZ, NZ) * 8 + lax.rem(xx + NX, NX) * 2 + cc, y)

    mate = (r + 1 - 2 * c, y)
    up_dev, down_dev = at(z + 1, x, c), at(z - 1, x, c)

    def rcopy(src, dst, ss, rs, dev):
        return pltpu.make_async_remote_copy(
            src_ref=src, dst_ref=dst, send_sem=ss, recv_sem=rs, device_id=dev, device_id_type=MESH
        )

    cut, ff = wg.shape[4], hidden.shape[1]
    loads = [
        (qa, q.at[x, :, 0:128]),
        (qb, q.at[x, :, 128:256]),
        (ka, kv.at[z, c, :, 0:128]),
        (kb, kv.at[z, c, :, 128:256]),
        (va, kv.at[z, c, :, 256:512]),
        (gw.at[:, 0:cut], wg.at[z, x, c]),
        (gw.at[:, cut:ff], wu.at[z, x, c, :, 0 : ff - cut]),
        (uw, wu.at[z, x, c, :, ff - cut : 2 * ff - cut]),
        (out_w, ow.at[y]),
        (res_in, res),
        (down_w, dw),
    ]
    loads = [pltpu.make_async_copy(s, d, loc.at[i]) for i, (s, d) in enumerate(loads)]
    for d in loads:
        d.start()
    barrier = pltpu.get_barrier_semaphore()
    across = [(r, lax.rem(y + d, NY)) for d in DX]
    after, before = (lax.rem(r + 1, 64), y), (lax.rem(r + 63, 64), y)
    greeted = [up_dev, down_dev, mate, after, before] + [at(z, x + d, c) for d in DX] + across
    for dev in greeted:
        pl.semaphore_signal(barrier, inc=1, device_id=dev, device_id_type=MESH)
    pl.semaphore_wait(barrier, len(greeted))
    for d in loads[:5]:
        d.wait()

    def q_copy(i, slot):
        return rcopy(q.at[slot], q.at[slot], snd.at[0], one.at[0], at(z, x + DX[i], c))

    plus_n, minus_n = 4 - c, 3 + c

    def z_ring(ref_at, sends, recvs):
        def plus(s):
            blk = lax.rem(z - s + 1 + NZ, NZ)
            return rcopy(ref_at(blk), ref_at(blk), sends, recvs.at[0, s - 1], up_dev)

        def minus(s):
            blk = lax.rem(z + s - 1, NZ)
            return rcopy(ref_at(blk), ref_at(blk), sends, recvs.at[1, s - 1], down_dev)

        def plus_in(s):
            blk = lax.rem(z - s + NZ, NZ)
            return rcopy(ref_at(blk), ref_at(blk), sends, recvs.at[0, s - 1], up_dev)

        def minus_in(s):
            blk = lax.rem(z + s, NZ)
            return rcopy(ref_at(blk), ref_at(blk), sends, recvs.at[1, s - 1], down_dev)

        return plus, minus, plus_in, minus_in

    def only(n, s, fn):
        if s <= 3:
            fn()
        elif s == 4:
            pl.when(n == 4)(fn)

    kv_rings = [
        z_ring(lambda b, h=h: kv.at[b, c, h * 96 : (h + 1) * 96], snd.at[1], kvr.at[h])
        for h in range(2)
    ]
    wu_ring = z_ring(lambda b: wu.at[b, x, c], snd.at[2], wur)
    wg_rings = [
        z_ring(lambda b, j=j: wg.at[b, lax.rem(x + j, NX), c], snd.at[3], gzr.at[j])
        for j in range(NX)
    ]

    def wg_step(j, s):
        ring_step(wg_rings[j], s, lambda k: None)
        if j == NX - 1:
            for k in ks(s):
                wg_hand(k, c).start()


    def hand_blk(k):
        off = (0, -1, -2, -3, 1, 2, 3, 4)[k]
        return lax.rem(z + off + NZ, NZ)

    def kv_hand(k, lane):
        b = hand_blk(k)
        return rcopy(kv.at[b, lane], kv.at[b, lane], snd.at[4], kdr.at[k], mate)

    def wg_hand(k, lane):
        b = hand_blk(k)
        return rcopy(wg.at[b, :, lane], wg.at[b, :, lane], snd.at[5], gdr.at[k], mate)

    def wu_hand(k, lane):
        b = hand_blk(k)
        return rcopy(wu.at[b, :, lane], wu.at[b, :, lane], snd.at[6], wdr.at[k], mate)

    toward = 1 - 2 * c

    def wu_x(k, d):
        ref = wu.at[hand_blk(k), x, c]
        return rcopy(ref, ref, snd.at[7], wxr.at[k, 0], at(z, x + d, c))

    def wu_x2(k):
        ref = wu.at[hand_blk(k), lax.rem(x - toward + NX, NX), c]
        return rcopy(ref, ref, snd.at[8], wxr.at[k, 1], at(z, x + toward, c))

    def wg_x(i, xx):
        return rcopy(wg.at[z, xx, c], wg.at[z, xx, c], snd.at[9], one.at[1], at(z, x + DX[i], c))

    def got(ref, sem):
        rcopy(ref, ref, snd.at[0], sem, mate).wait_recv()

    def gone(ref, n):
        rcopy(ref, ref, snd.at[n], one.at[0], mate).wait_send()

    def from_x(i):
        return lax.rem(x - DX[i] + NX, NX)

    def ring_start(ring):
        ring[0](1).start()
        ring[1](1).start()

    def ring_step(ring, s, hand):
        def p():
            ring[2](s).wait_recv()
            only(plus_n, s + 1, lambda: ring[0](s + 1).start())
            if s < 4:
                hand(s)
            else:
                hand(7)

        def n():
            ring[3](s).wait_recv()
            only(minus_n, s + 1, lambda: ring[1](s + 1).start())
            if s < 4:
                hand(3 + s)
            else:
                hand(7)

        only(plus_n, s, p)
        only(minus_n, s, n)

    def ks(s):
        return (s, 3 + s) if s < 4 else (7,)

    def from_y(i):
        return lax.rem(y - DX[i] + NY, NY)

    half_cols = ow.shape[2] // 2

    def ow_y(i, yy):
        ref = ow.at[yy, :, pl.ds(pl.multiple_of(c * half_cols, 128), half_cols)]
        return rcopy(ref, ref, snd.at[10], one.at[2], across[i])

    def ow_hand(i, lane):
        ref = ow.at[from_y(i), :, pl.ds(pl.multiple_of(lane * half_cols, 128), half_cols)]
        return rcopy(ref, ref, snd.at[11], one.at[3], mate)

    def heads_y(i, yy):
        return rcopy(heads.at[yy], heads.at[yy], snd.at[12], hsr.at[i], across[i])

    def edge_copy():
        return rcopy(edge_out, edge_in, snd.at[13], one.at[5], after)

    def down_y(i, n):
        return rcopy(
            part.at[n, across[i][1]], drecv.at[i, n], snd.at[14], dyr.at[n], across[i]
        )

    for i in range(3):
        q_copy(i, x).start()
    ring_start(kv_rings[0])
    ring_start(kv_rings[1])
    kv_hand(0, c).start()
    for d in loads[5:9]:
        d.wait()
    for i in range(3):
        ow_y(i, y).start()
    ring_start(wu_ring)

    lane = lax.broadcasted_iota(jnp.int32, (ROWS, 128), 1)

    def prepare(slot):
        for half in range(2):
            block = q[slot, :, half * 128 : (half + 1) * 128] * bf16(0.125)
            zero = jnp.zeros_like(block)
            qz[half, slot, 0:ROWS] = jnp.where(lane < 64, block, zero)
            qz[half, slot, ROWS : 2 * ROWS] = jnp.where(lane < 64, zero, block)

    prepare(x)
    ring_step(kv_rings[0], 1, lambda k: None)
    for i in range(3):
        wg_x(i, x).start()
    wu_x(0, 1).start()
    wu_x(0, 3).start()
    ring_step(kv_rings[1], 1, lambda k: kv_hand(k, c).start())
    got(q.at[0:3], one.at[0])
    for i in range(3):
        prepare(from_x(i))

    def piece(chunk, pair, slot, masked):
        if masked:
            j = lax.broadcasted_iota(jnp.int32, (1, 768), 1)
            second = (j >= 384).astype(jnp.int32)
            core = ((j - 384 * second) >= 192).astype(jnp.int32)
            off = j - 384 * second - 192 * core
            key_pos = ((2 * pair + second) * 8 + x * 2 + core) * ROWS + off
            i = lax.broadcasted_iota(jnp.int32, (2 * ROWS, 1), 0)
            i = i - ROWS * (i >= ROWS).astype(jnp.int32)
            query_pos = (z * 8 + slot * 2 + c) * ROWS + i
            visible = key_pos <= query_pos
        for half in range(2):
            keys = kv[pl.ds(2 * pair, 2), :, :, half * 128 : (half + 1) * 128].reshape(768, 128)
            s = lax.dot_general(
                qz[half, slot], keys, (((1,), (1,)), ((), ())), preferred_element_type=f32
            )
            if masked:
                s = jnp.where(visible, s, HIDE)
            new = jnp.broadcast_to(
                jnp.maximum(jnp.max(s, axis=1, keepdims=True), FLOOR), (2 * ROWS, 128)
            )
            m[chunk, half, slot] = new
            e = jnp.exp(s - new[:, 0:1])
            part_sum = e[:, 0:128]
            for t in range(1, 6):
                part_sum = part_sum + e[:, t * 128 : (t + 1) * 128]
            l[chunk, half, slot] = part_sum
            eb = e.astype(bf16)
            for h in range(2):
                rows = slice(h * ROWS, (h + 1) * ROWS)
                vals = kv[pl.ds(2 * pair, 2), :, :, 256 + h * 128 : 384 + h * 128].reshape(768, 128)
                acc[chunk, half, slot, rows] = jnp.dot(eb[rows], vals, preferred_element_type=f32)

    def unseen(chunk, slot):
        for half in range(2):
            m[chunk, half, slot] = jnp.full((2 * ROWS, 128), FLOOR, f32)
            l[chunk, half, slot] = jnp.zeros((2 * ROWS, 128), f32)
            acc[chunk, half, slot] = jnp.zeros((2 * ROWS, 128), f32)

    own = z // 2
    odd = z % 2
    pairs = (
        own,
        lax.rem(own + jnp.where(odd == 1, 1, 3), 4),
        lax.rem(own + jnp.where(odd == 1, 3, 1), 4),
        lax.rem(own + 2, 4),
    )

    def join(slot, take_values):
        st = jnp.zeros((ROWS, 128), f32)
        for half in range(2):
            for h in range(2):
                rows = slice(h * ROWS, (h + 1) * ROWS)
                k = half * 2 + h
                ms = [m[n, half, slot, rows] for n in range(4)]
                top = jnp.maximum(jnp.maximum(ms[0], ms[1]), jnp.maximum(ms[2], ms[3]))
                tot, val = None, None
                for n in range(4):
                    w = jnp.exp(ms[n] - top)
                    t = l[n, half, slot, rows] * w
                    v = acc[n, half, slot, rows] * w
                    tot, val = (t, v) if n == 0 else (tot + t, val + v)
                take_values(half, h, val)
                st = jnp.where(lane == k, top, st)
                st = jnp.where(lane == 4 + k, jnp.sum(tot, axis=1, keepdims=True), st)
        return st

    def p_copy(i):
        return rcopy(psend.at[i], precv.at[i], snd.at[15], one.at[6], (at(z, x + i_dx(i), c)))

    def s_copy(i):
        return rcopy(ssend.at[i], srecv.at[i], snd.at[16], one.at[7], (at(z, x + i_dx(i), c)))

    def i_dx(i):
        return jnp.where(i == 0, 2, jnp.where(i == 1, 1, 3))

    def wu_spread(k):
        wu_x(k, 1).start()
        wu_x(k, 3).start()

    def wu_mid(k):
        got(wu.at[0, 0:2, c], wxr.at[k, 0])
        wu_x2(k).start()

    def wu_finish(k):
        got(wu.at[0, 0, c], wxr.at[k, 1])
        wu_hand(k, c).start()

    def kv_arrive(s, h):
        ring_step(kv_rings[h], s, lambda k: kv_hand(k, c).start() if h == 1 else None)

    def wu_arrive(s, spread):
        ring_step(wu_ring, s, lambda k: None)
        for k in spread:
            wu_spread(k)

    def all_slots(chunk, masked, first, s):
        pair = pairs[chunk]

        def body(slot, carry):
            if masked:
                piece(chunk, pair, slot, True)
            else:
                seen = pair < own
                pl.when(seen)(lambda: piece(chunk, pair, slot, False))
                pl.when(jnp.logical_not(seen))(lambda: unseen(chunk, slot))
            pl.when(slot == 0)(first)
            pl.when(slot == 1)(lambda: kv_arrive(s, 0))
            pl.when(slot == (3 if masked else 2))(lambda: kv_arrive(s, 1))
            return carry

        lax.fori_loop(0, NX, body, 0)

    for k in (0,) + ks(1):
        kv_hand(k, 1 - c).wait_recv()
    all_slots(0, True, lambda: wu_arrive(1, ks(1)), 2)
    got(wg.at[0, 0:3, c], one.at[1])
    wg_hand(0, c).start()
    wu_mid(0)
    for k in ks(2):
        kv_hand(k, 1 - c).wait_recv()
    all_slots(1, False, lambda: wu_arrive(2, ks(2)), 3)
    for k in ks(3):
        kv_hand(k, 1 - c).wait_recv()

    def last(idx, carry):
        final = jnp.logical_and(idx >= 3, idx != 6)
        i = jnp.where(idx < 3, idx, jnp.where(idx < 6, idx - 3, 3))
        slot = lax.rem(x + jnp.where(i == 3, 0, i_dx(i)), NX)
        chunk = jnp.where(final, 3, 2)
        pair = jnp.where(final, pairs[3], pairs[2])

        @pl.when(idx == 3)
        def _():
            for k in ks(4):
                kv_hand(k, 1 - c).wait_recv()

        seen = pair < own
        pl.when(seen)(lambda: piece(chunk, pair, slot, False))
        pl.when(jnp.logical_not(seen))(lambda: unseen(chunk, slot))

        @pl.when(jnp.logical_and(final, i < 3))
        def _():
            def put(half, h, val):
                col = (half * 2 + h) * 128
                psend[i, :, col : col + 128] = val.astype(bf16)

            st = jnp.concatenate((join(slot, put), jnp.zeros((64, 128), f32)), axis=0)
            ssend[i] = st.T[0:8]
            p_copy(i).start()
            s_copy(i).start()

        @pl.when(idx == 0)
        def _():
            wu_arrive(3, ())
            for ring in wg_rings:
                ring_start(ring)

        @pl.when(idx == 1)
        def _():
            wu_finish(0)
            for k in ks(1):
                wu_mid(k)

        @pl.when(idx == 2)
        def _():
            kv_arrive(4, 0)
            kv_arrive(4, 1)
            for k in ks(2):
                wu_mid(k)

        @pl.when(idx == 3)
        def _():
            wu_arrive(4, ())
            wg_step(0, 1)

        for j in (1, 2, 3):
            @pl.when(idx == 3 + j)
            def _():
                wg_step(j, 1)

        @pl.when(idx == 5)
        def _():
            for k in ks(1):
                wu_finish(k)

        @pl.when(idx == 6)
        def _():
            for k in ks(2):
                wu_finish(k)

        @pl.when(idx == 7)
        def _():
            wg_step(0, 2)

        return carry

    lax.fori_loop(0, 8, last, 0)
    for k in (3, 6, 7):
        wu_spread(k)
    wg_step(1, 2)
    wg_step(2, 2)
    wg_step(3, 2)
    got(ow.at[0:3, :, 0:half_cols], one.at[2])
    for i in range(3):
        ow_hand(i, c).start()

    def take(i):
        st = jnp.concatenate((srecv[i], jnp.zeros((120, 256), f32)), axis=0).T[0:ROWS]
        return st

    mine = {}

    def keep(half, h, val):
        mine[half, h] = val

    stats = [join(x, keep)]
    got(precv, one.at[6])
    got(srecv, one.at[7])
    stats += [take(i) for i in range(3)]
    for h in range(2):
        parts = []
        for half in range(2):
            k = half * 2 + h
            col = k * 128
            ms = [st[:, k : k + 1] for st in stats]
            ls = [st[:, 4 + k : 5 + k] for st in stats]
            top = functools.reduce(jnp.maximum, ms)
            ws = [jnp.exp(a - top) for a in ms]
            tot = sum(w * t for w, t in zip(ws, ls))
            joined = mine[half, h] * ws[0]
            for i in range(3):
                joined = joined + precv[i, :, col : col + 128].astype(f32) * ws[i + 1]
            parts.append(joined / tot)
        diff = parts[0] - lam[h] * parts[1]
        heads[y, :, h * 128 : (h + 1) * 128] = rms_scale(diff, gain[...]).astype(bf16)

    for i in range(3):
        heads_y(i, y).start()

    wg_step(0, 3)
    wu_mid(3)
    wg_step(1, 3)
    wg_step(2, 3)
    wg_step(3, 3)
    wu_mid(6)

    loads[9].wait()
    loads[10].wait()
    got(ow.at[0:3, :, 0:half_cols], one.at[3])
    width = stream.shape[2]
    for i in (None, 1, 2, 0):
        yy = y
        if i is not None:
            yy = from_y(i)
            heads_y(i, yy).wait_recv()
        for n in range(0, width, 512):
            cols = slice(n, n + 512)
            more = jnp.dot(heads[yy], ow[yy, :, cols], preferred_element_type=f32)
            more = more.reshape(NY, ROWS // NY, 512)
            if i is None:
                more = more + res[:, cols].astype(f32).reshape(NY, ROWS // NY, 512)
            else:
                more = more + stream[:, :, cols]
            stream[:, :, cols] = more
    wu_mid(7)
    rows = stream[...].reshape(ROWS, width)
    normed = rms_scale(rows, mix_gain[...]).astype(bf16)
    for zz in range(NZ):
        ffn[zz] = normed[:, zz * 256 : (zz + 1) * 256]

    order = (0,) + ks(1) + ks(2) + ks(3) + ks(4)
    pieces = ((wg, slice(0, cut)), (wu, slice(cut, 2 * ff)))
    for n in range(0, 8, 2):
        two = order[n : n + 2]
        if n == 0:
            wg_step(0, 4)
        if n == 2:
            wg_step(1, 4)
            wg_step(2, 4)
            wu_finish(3)
        if n == 4:
            wu_finish(6)
            wg_step(3, 4)
            wu_finish(7)
        for k in two:
            wg_hand(k, 1 - c).wait_recv()
            wu_hand(k, 1 - c).wait_recv()
        blks = [hand_blk(k) for k in two]

        def product(w, top):
            return sum(
                jnp.dot(ffn[b, top:], w[b].reshape(256, -1), preferred_element_type=f32)
                for b in blks
            )

        if n == 6:
            for w, cols in pieces:
                tip = product(w, ROWS - 16)
                tip = (tip[8:] + pad[ROWS : 8 + ROWS, cols]).astype(bf16).astype(f32)
                edge_out[:, cols] = tip[6:8]
            edge_copy().start()
        for w, cols in pieces:
            pre = product(w, 0)
            if n > 0:
                pre = pre + pad[8 : 8 + ROWS, cols]
            if n == 6:
                pre = pre.astype(bf16).astype(f32)
            pad[8 : 8 + ROWS, cols] = pre

    def mix(top, size):
        for n in range(0, ff, 128):
            cols = slice(n, n + 128)
            conv = []
            for base, taps in ((0, gate_taps), (ff, up_taps)):
                there = slice(base + n, base + n + 128)
                v = taps[0:1, cols] * pad[6 + top : 6 + top + size, there]
                v = v + taps[1:2, cols] * pad[7 + top : 7 + top + size, there]
                v = v + taps[2:3, cols] * pad[8 + top : 8 + top + size, there]
                conv.append(v)
            hidden[top : top + size, cols] = (jax.nn.silu(conv[0]) * conv[1]).astype(bf16)

    mix(16, ROWS - 16)
    edge_copy().wait_recv()
    pad[6:8, :] = jnp.where(r == 0, 0.0, edge_in[...])
    mix(0, 16)

    for n in range(NY):
        cols = slice(n * 512, (n + 1) * 512)
        down = jnp.dot(hidden[...], dw[:, cols], preferred_element_type=f32)
        part[n] = down.astype(bf16).reshape(NY, ROWS // NY, 512)
        for i in range(3):
            down_y(i, n).start()
    edge_copy().wait_send()
    gone(q.at[0:3], 0)
    gone(kv.at[0:7, 0], 1)
    gone(wu.at[0:7, 0, 0], 2)
    gone(wg.at[0:7, :, 0], 3)
    gone(kv.at[:, 0], 4)
    gone(wg.at[:, :, 0], 5)
    gone(wu.at[:, :, 0], 6)
    gone(wu.at[:, 0:2, 0], 7)
    gone(wu.at[:, 0, 0], 8)
    gone(wg.at[0, 0:3, 0], 9)
    gone(ow.at[0:3, :, 0:half_cols], 10)
    gone(ow.at[0:3, :, 0:half_cols], 11)
    gone(heads.at[0:3], 12)
    gone(psend, 15)
    gone(ssend, 16)
    for n in range(NY):
        cols = slice(n * 512, (n + 1) * 512)
        total = stream[y, :, cols] + part[n, y].astype(f32)
        got(drecv.at[:, n], dyr.at[n])
        for i in range(3):
            total = total + drecv[i, n].astype(f32)
        out[:, cols] = total.astype(bf16)
    gone(drecv, 14)


def layer(*args):
    ANY = pl.BlockSpec(memory_space=pl.ANY)
    VM = pl.BlockSpec(memory_space=pltpu.VMEM)
    SM = pl.BlockSpec(memory_space=pltpu.SMEM)
    ff, width = args[5].shape[1], args[8].shape[1]
    dma = pltpu.SemaphoreType.DMA
    cut = 8 * 128 if ff > 8 * 128 else ff // 2
    sems = [(11,), (17,), (8,), (3,), (2, 2, 4), (8,), (2, 4), (8, 2), (8,), (NX, 2, 4), (8,), (NY,)]
    return pl.pallas_call(
        layer_kernel,
        out_shape=jax.ShapeDtypeStruct((ROWS // NY, width), bf16),
        in_specs=[ANY] * 10 + [SM] + [VM] * 4,
        out_specs=VM,
        scratch_shapes=[
            pltpu.VMEM((4, ROWS, 256), bf16),
            pltpu.VMEM((8, 2, ROWS, 512), bf16),
            pltpu.VMEM((8, 4, 2, 32, cut), bf16),
            pltpu.VMEM((8, 4, 2, 32, 2 * ff - cut), bf16),
            pltpu.VMEM((2, 4, 2 * ROWS, 128), bf16),
            pltpu.VMEM((4, 2, 4, 2 * ROWS, 128), f32),
            pltpu.VMEM((4, 2, 4, 2 * ROWS, 128), f32),
            pltpu.VMEM((4, 2, 4, 2 * ROWS, 128), f32),
            pltpu.VMEM((3, ROWS, 512), bf16),
            pltpu.VMEM((3, ROWS, 512), bf16),
            pltpu.VMEM((3, 8, 256), f32),
            pltpu.VMEM((3, 8, 256), f32),
            pltpu.VMEM((NY, ROWS, 256), bf16),
            pltpu.VMEM((NY, 256, width), bf16),
            pltpu.VMEM((ff, width), bf16),
            pltpu.VMEM((ROWS, width), bf16),
            pltpu.VMEM((NY, ROWS // NY, width), f32),
            pltpu.VMEM((NZ, ROWS, 256), bf16),
            pltpu.VMEM((8 + ROWS, 2 * ff), f32),
            pltpu.VMEM((ROWS, ff), bf16),
            pltpu.VMEM((2, 2 * ff), f32),
            pltpu.VMEM((2, 2 * ff), f32),
            pltpu.VMEM((NY, NY, ROWS // NY, 512), bf16),
            pltpu.VMEM((3, NY, ROWS // NY, 512), bf16),
        ] + [dma(s) for s in sems],
        compiler_params=pltpu.CompilerParams(
            collective_id=0, has_side_effects=True, vmem_limit_bytes=63 * 1024 * 1024
        ),
        name="layer",
    )(*args)


def shards(
    q_first, k_first, q_second, k_second, values, lambdas, head_gain, out_weight, residual_in,
    mix_gain, gate_weight, up_weight, gate_taps, up_taps, down_weight,
):
    return layer(
        q_first, q_second, k_first, k_second, values, gate_weight, up_weight, out_weight,
        residual_in, down_weight, lambdas, head_gain[None], mix_gain[None], gate_taps, up_taps,
    )


def solution(mesh):
    in_specs = (
        P("sp", "tp"), P("sp", "tp"), P("sp", "tp"), P("sp", "tp"), P("sp", "tp"),
        P("tp"), P(), P("tp", None), P("sp", None), P(),
        P("sp", "tp"), P("sp", "tp"), P(None, "tp"), P(None, "tp"), P("tp", None),
    )
    out_specs = P(("sp", "tp"), None)
    return jax.shard_map(shards, mesh=mesh, in_specs=in_specs, out_specs=out_specs, check_vma=False)
```
